32 devices in a mesh: grp: 2 (over y), ep: 16 (over z, x, core), tp: 1.
Axes of the slice: x: 2, y: 2, z: 4, core: 2. Of those that a mesh axis runs over, the one named last changes fastest.
Arguments:
- tokens: bfloat16 [3072, 2048], P(('grp', 'ep')), parts along dimension 0, may hold values from -6 to 6
- prior_state: float32 [2, 3072, 4096], P(None, ('grp', 'ep'), 'tp'), parts along dimension 1, may hold values from -6 to 6
- mix_gain: float32 [2048], replicated, may hold values from 0.1 to 1.9
- in_weight: bfloat16 [2048, 1024], P(None, 'tp'), may hold values from -0.125 to 0.125
- decay_rate: float32 [64, 64], P('tp'), may hold values from 0.2 to 20
- frequency: float32 [64, 64], P('tp'), may hold values from 0 to 12
- log_step: float32 [64], P('tp'), may hold values from -4.6 to 0
- input_map: float32 [2, 64, 64, 16], P(None, 'tp'), may hold values from -6 to 6
- output_map: float32 [2, 64, 16, 64], P(None, 'tp'), may hold values from -0.5 to 0.5
- skip_gain: float32 [1024], P('tp'), may hold values from -4 to 4
- out_weight: bfloat16 [1024, 2048], P('tp'), may hold values from -0.1875 to 0.1875
- channel_gain: float32 [2048], replicated, may hold values from 0.1 to 1.9
- expert_gate: bfloat16 [16, 2048, 512], P('ep', None, 'tp'), may hold values from -0.125 to 0.125
- expert_up: bfloat16 [16, 2048, 512], P('ep', None, 'tp'), may hold values from -0.125 to 0.125
- expert_down: bfloat16 [16, 512, 2048], P('ep', 'tp'), may hold values from -0.25 to 0.25
- shared_gate: bfloat16 [2048, 512], P(None, 'tp'), may hold values from -0.125 to 0.125
- shared_up: bfloat16 [2048, 512], P(None, 'tp'), may hold values from -0.125 to 0.125
- shared_down: bfloat16 [512, 2048], P('tp'), may hold values from -0.25 to 0.25
- routes: int32 [3072, 6], P(('grp', 'ep')), parts along dimension 0, may hold values from 0 to 15, all different within a row; in each aligned block of 96 rows (0 to 95, 96 to 191, ...) at most 54 rows name the same one
- route_weights: float32 [3072, 6], P(('grp', 'ep')), parts along dimension 0, may hold values from 0.05 to 0.8
Outputs:
- layer_out: bfloat16 [3072, 2048], P(('grp', 'ep'), 'tp'), parts along dimension 0
- new_state: float32 [2, 3072, 4096], P(None, ('grp', 'ep'), 'tp'), parts along dimension 1
The draws below stay inside these ranges and needn't reach their ends.
There are 2 independent parts, one for each index of `grp`. The reference program is written for one: setup_inputs(seed, part) draws one part's arguments, and reference() takes and returns one part's arrays. A program takes and returns all parts, laid end to end along the dimension named above; an argument that names none is the same for every part. Nothing has to cross between parts.
Inputs may be any that keep to these rules, and one draw needn't show every extreme that they name: `routes`: each row names 6 different experts; among the rows of one index of ep no expert is named by more than 54 rows.
All inputs are finite; a program needn't handle non-finite values.
Results may differ from the reference program's by a relative error of at most 0.017.
Values may be sent and summed in bfloat16 or wider, within the bound.
A program may use at most 128 MiB of HBM per device.

```python
import math
import jax
import jax.numpy as jnp
import numpy as np
from jax import lax

D = 2048
SSM_WIDTH = 1024
GROUPS = 64
GROUP_WIDTH = 16
STATE = 64
EXP_WIDTH = 512
SHARED_WIDTH = 512
TOPK = 6
SEQ_DEV = 96
SEQS = 1536
EXPERTS = 16
CAP = 54
N_EP = 16
N_TP = 1


def block_levels(stream_key, extent, pieces, smallest, high):
    def one(position, blocks):
        heights = jax.random.uniform(jax.random.fold_in(jax.random.fold_in(stream_key, 6), position), (blocks,), jnp.float32, smallest / len(pieces), high / len(pieces))
        return jnp.repeat(jnp.exp(heights), extent[position] // blocks).reshape((-1,) + (1,) * (len(extent) - position - 1))

    factor_of = one(*pieces[0])
    for cut in pieces[1:]:
        factor_of = factor_of * one(*cut)
    return factor_of


def deal_out(rng, own, number, rows, number_of, top, reach, skew):
    order = jax.random.permutation(rng, number_of)
    packed, ordinary = shares(number_of, rows * top, reach, skew, True), shares(number_of, rows * top, reach, skew, False)
    places = jnp.arange(number_of)

    def named(sizes, offset_by):
        used = int((sizes > 0).sum())
        fixed = max(1, used // 4)
        passed = fixed + (places - fixed + offset_by * (used - fixed)) % max(1, number_of - fixed)
        return jnp.zeros((number_of,), jnp.int32).at[order[jnp.where(places < fixed, places, passed)]].set(jnp.asarray(sizes, jnp.int32))

    sizes = jnp.where(number % 4 == 0, named(packed, number // 4), named(ordinary, number - number // 4 - 1))
    mixed = jax.random.permutation(jax.random.fold_in(own, 3), number_of)
    donor, receiver = mixed[0:number_of // 2 * 2:2], mixed[1:number_of // 2 * 2:2]
    margin = jnp.minimum(sizes[donor] - 1, reach - sizes[receiver]) // 2
    margin = jnp.where((donor == order[0]) | (receiver == order[0]) | (sizes[receiver] == 0), 0, jnp.maximum(margin, 0))
    passed = jax.random.randint(jax.random.fold_in(own, 4), (number_of // 2,), 0, 1 << 20) % (margin + 1)
    sizes = sizes.at[donor].add(-passed).at[receiver].add(passed)
    labels = jnp.searchsorted(jnp.cumsum(sizes), jnp.arange(rows * top), side="right").astype(jnp.int32)
    grid = labels.reshape(top, rows).T
    grid = grid[jax.random.permutation(jax.random.fold_in(own, 1), rows)]
    offset_by = jax.random.randint(jax.random.fold_in(own, 2), (rows, 1), 0, top)
    return jnp.take_along_axis(grid, (jnp.arange(top)[None, :] + offset_by) % top, axis=1)


def shares(amount, total, reach, slope, full):
    weights = [(1 << 20) // math.isqrt(rank ** slope) + 1 for rank in range(1, amount + 1)]
    largest = reach if full else min(reach, max(-(-total // amount), total * weights[0] // sum(weights)))
    least = 1 if total - largest >= amount - 1 else 0
    counts, spare = [largest] + [least] * (amount - 1), total - largest - least * (amount - 1)
    while spare > 0:
        free = [i for i in range(1, amount) if counts[i] < largest] or [i for i in range(1, amount) if counts[i] < reach]
        mass, left = sum([weights[i] for i in free]), spare
        for i in free:
            more = min(reach - counts[i], max(1, left * weights[i] // mass), spare)
            counts[i] = counts[i] + more
            spare = spare - more
    return np.array(counts)


def gaussian(key, dims, spread, most, shards=(), held_as=jnp.bfloat16):
    drawn = spread * jax.random.normal(key, dims, jnp.float32)
    if shards:
        drawn = drawn * block_levels(key, dims, shards, -0.22, 0.18)
    return jnp.clip(drawn, -most, most).astype(held_as)


def setup_inputs(seed: int = 0, part: int = 0) -> dict:
    keys = jax.random.split(jax.random.key(seed), 21)
    part_keys = jax.random.split(jax.random.fold_in(keys[20], part), 21)
    tokens = gaussian(part_keys[0], (SEQS, D), 1.0, 6.0, ((0, 16),))
    prior_state = gaussian(part_keys[1], (2, SEQS, GROUPS * STATE), 1.0, 6.0, ((1, 16),), jnp.float32)
    mix_gain = jnp.clip(1.0 + 0.18 * jax.random.normal(keys[2], (D,), jnp.float32), 0.1, 1.9)
    in_weight = gaussian(keys[3], (D, SSM_WIDTH), D ** -0.5, 0.125)
    decay_rate = jnp.clip(jnp.exp(jax.random.uniform(keys[4], (GROUPS, STATE), jnp.float32, math.log(0.2), math.log(20.0))), 0.2, 20.0)
    frequency = jnp.clip(jax.random.uniform(keys[5], (GROUPS, STATE), jnp.float32, 0.0, 12.0), 0.0, 12.0)
    log_step = jnp.clip(jax.random.uniform(keys[6], (GROUPS,), jnp.float32, -4.6, 0.0), -4.6, 0.0)
    input_map = gaussian(keys[7], (2, GROUPS, STATE, GROUP_WIDTH), 1.0, 6.0, (), jnp.float32)
    output_map = gaussian(keys[8], (2, GROUPS, GROUP_WIDTH, STATE), (2 * STATE) ** -0.5, 0.5, (), jnp.float32)
    skip_gain = gaussian(keys[9], (SSM_WIDTH,), 1.0, 4.0, (), jnp.float32)
    out_weight = gaussian(keys[10], (SSM_WIDTH, D), SSM_WIDTH ** -0.5, 0.1875)
    channel_gain = jnp.clip(1.0 + 0.18 * jax.random.normal(keys[11], (D,), jnp.float32), 0.1, 1.9)
    expert_gate = gaussian(keys[12], (EXPERTS, D, EXP_WIDTH), D ** -0.5, 0.125, ((0, 16),))
    expert_up = gaussian(keys[13], (EXPERTS, D, EXP_WIDTH), D ** -0.5, 0.125, ((0, 16),))
    expert_down = gaussian(keys[14], (EXPERTS, EXP_WIDTH, D), EXP_WIDTH ** -0.5, 0.25, ((0, 16),))
    shared_gate = gaussian(keys[15], (D, SHARED_WIDTH), D ** -0.5, 0.125)
    shared_up = gaussian(keys[16], (D, SHARED_WIDTH), D ** -0.5, 0.125)
    shared_down = gaussian(keys[17], (SHARED_WIDTH, D), SHARED_WIDTH ** -0.5, 0.25)
    routes_keys = jax.random.split(jax.random.fold_in(part_keys[18], 1), SEQS // SEQ_DEV)
    routes_turns = jax.random.permutation(jax.random.fold_in(part_keys[18], 3), SEQS // SEQ_DEV)
    routes = jax.vmap(lambda own, number: deal_out(jax.random.fold_in(part_keys[18], 2), own, number, SEQ_DEV, EXPERTS, TOPK, CAP, 2))(routes_keys, routes_turns).reshape((SEQS, TOPK))
    route_weights = jnp.clip(0.05 + 0.75 * jax.random.uniform(part_keys[19], (SEQS, TOPK), jnp.float32) ** block_levels(part_keys[19], (SEQS, TOPK), ((0, 16),), -0.2, 0.2), 0.05, 0.8)
    return {"tokens": tokens, "prior_state": prior_state, "mix_gain": mix_gain, "in_weight": in_weight, "decay_rate": decay_rate, "frequency": frequency, "log_step": log_step, "input_map": input_map, "output_map": output_map, "skip_gain": skip_gain, "out_weight": out_weight, "channel_gain": channel_gain, "expert_gate": expert_gate, "expert_up": expert_up, "expert_down": expert_down, "shared_gate": shared_gate, "shared_up": shared_up, "shared_down": shared_down, "routes": routes, "route_weights": route_weights}


norm_eps = 1e-06
highest = lax.Precision.HIGHEST

def root_scale(activations, scale_gain):
    values = activations.astype(jnp.float32)
    factor = lax.rsqrt(lax.optimization_barrier(jnp.mean(values * values, axis=-1, keepdims=True)) + norm_eps)
    return (values * factor * scale_gain).astype(jnp.bfloat16)

def state_update(drive_rows, prior_state, decay_rate, frequency, log_step, input_map, output_map, skip_gain):
    sequences = drive_rows.shape[0]
    groups = decay_rate.shape[0]
    driven = drive_rows.astype(jnp.float32).reshape(sequences, groups, -1)
    step_size = jnp.exp(log_step)[:, None]
    real_rate = -decay_rate
    magnitude = jnp.exp(real_rate * step_size)
    turn_real = magnitude * jnp.cos(frequency * step_size)
    turn_imag = magnitude * jnp.sin(frequency * step_size)
    denominator = real_rate * real_rate + frequency * frequency
    hold_real = ((turn_real - 1.0) * real_rate + turn_imag * frequency) / denominator
    hold_imag = (turn_imag * real_rate - (turn_real - 1.0) * frequency) / denominator
    push_real = jnp.einsum('sgh,gph->sgp', driven, input_map[0], precision=highest)
    push_imag = jnp.einsum('sgh,gph->sgp', driven, input_map[1], precision=highest)
    enter_real = push_real * hold_real - push_imag * hold_imag
    enter_imag = push_real * hold_imag + push_imag * hold_real
    old_real = prior_state[0].reshape(sequences, groups, -1)
    old_imag = prior_state[1].reshape(sequences, groups, -1)
    fresh_real = turn_real * old_real - turn_imag * old_imag + enter_real
    fresh_imag = turn_real * old_imag + turn_imag * old_real + enter_imag
    readout = jnp.einsum('ghp,sgp->sgh', output_map[0], fresh_real, precision=highest)
    readout = readout - jnp.einsum('ghp,sgp->sgh', output_map[1], fresh_imag, precision=highest)
    readout = readout.reshape(sequences, -1) + skip_gain * drive_rows.astype(jnp.float32)
    fresh = jnp.stack([fresh_real.reshape(sequences, -1), fresh_imag.reshape(sequences, -1)])
    return (readout, fresh)

def split_block(activations, gate_weight, up_weight, down_weight):
    col_width = gate_weight.shape[1] // N_TP
    summed = jnp.zeros((activations.shape[0], down_weight.shape[1]), jnp.float32)
    for portion in range(N_TP):
        lower = portion * col_width
        gate_val = jnp.dot(activations, gate_weight[:, lower:lower + col_width], preferred_element_type=jnp.float32)
        up_val = jnp.dot(activations, up_weight[:, lower:lower + col_width], preferred_element_type=jnp.float32)
        hidden = (jax.nn.silu(gate_val) * up_val).astype(jnp.bfloat16)
        piece = jnp.dot(hidden, down_weight[lower:lower + col_width], preferred_element_type=jnp.float32)
        summed = summed + lax.optimization_barrier(piece.astype(jnp.bfloat16)).astype(jnp.float32)
    return summed

def reference(tokens, prior_state, mix_gain, in_weight, decay_rate, frequency, log_step, input_map, output_map, skip_gain, out_weight, channel_gain, expert_gate, expert_up, expert_down, shared_gate, shared_up, shared_down, routes, route_weights):
    normed = root_scale(tokens, mix_gain)
    drive_rows = jnp.dot(normed, in_weight, preferred_element_type=jnp.float32).astype(jnp.bfloat16)
    readout, new_state = state_update(drive_rows, prior_state, decay_rate, frequency, log_step, input_map, output_map, skip_gain)
    activated = jax.nn.gelu(readout).astype(jnp.bfloat16)
    col_width = out_weight.shape[0] // N_TP
    mixer_out = jnp.zeros((SEQS, D), jnp.float32)
    for portion in range(N_TP):
        lower = portion * col_width
        piece = jnp.dot(activated[:, lower:lower + col_width], out_weight[lower:lower + col_width], preferred_element_type=jnp.float32)
        mixer_out = mixer_out + lax.optimization_barrier(piece.astype(jnp.bfloat16)).astype(jnp.float32)
    middle = (tokens.astype(jnp.float32) + mixer_out).astype(jnp.bfloat16)
    second_normed = root_scale(middle, channel_gain)
    shared_out = split_block(second_normed, shared_gate, shared_up, shared_down)
    slot_limit = N_EP * CAP
    flat_routes = routes.reshape(-1)
    flat_weights = route_weights.reshape(-1)

    def one_expert(running, operands):
        expert_id, gate_weight, up_weight, down_weight = operands
        matched = flat_routes == expert_id
        chosen = jnp.nonzero(matched, size=slot_limit, fill_value=0)[0].astype(jnp.int32)
        found_count = jnp.sum(matched.astype(jnp.int32))
        is_valid = jnp.arange(slot_limit, dtype=jnp.int32) < found_count
        row_index = chosen // TOPK
        picked_rows = jnp.take(second_normed, row_index, axis=0)
        produced = split_block(picked_rows, gate_weight, up_weight, down_weight).astype(jnp.bfloat16)
        produced = lax.optimization_barrier(produced).astype(jnp.float32)
        weight_vals = jnp.where(is_valid, jnp.take(flat_weights, chosen), jnp.zeros_like(flat_weights[:1]))
        running = running.at[row_index].add(weight_vals[:, None] * produced)
        return (running, None)
    routed, _ = lax.scan(one_expert, jnp.zeros((SEQS, D), jnp.float32), (jnp.arange(EXPERTS, dtype=jnp.int32), expert_gate, expert_up, expert_down))
    layer_out = (middle.astype(jnp.float32) + routed + shared_out).astype(jnp.bfloat16)
    return (layer_out, new_state)
```

```python
import jax
import jax.numpy as jnp
from jax import lax
from jax.sharding import PartitionSpec as P

norm_eps = 1e-06
highest = lax.Precision.HIGHEST


def root_scale(activations, scale_gain):
    values = activations.astype(jnp.float32)
    factor = lax.rsqrt(jnp.mean(values * values, axis=-1, keepdims=True) + norm_eps)
    return (values * factor * scale_gain).astype(jnp.bfloat16)


def state_update(
    drive_rows, prior_state, decay_rate, frequency, log_step, input_map, output_map, skip_gain
):
    sequences = drive_rows.shape[0]
    groups = decay_rate.shape[0]
    driven = drive_rows.astype(jnp.float32).reshape(sequences, groups, -1)
    step_size = jnp.exp(log_step)[:, None]
    real_rate = -decay_rate
    magnitude = jnp.exp(real_rate * step_size)
    turn_real = magnitude * jnp.cos(frequency * step_size)
    turn_imag = magnitude * jnp.sin(frequency * step_size)
    denominator = real_rate * real_rate + frequency * frequency
    hold_real = ((turn_real - 1.0) * real_rate + turn_imag * frequency) / denominator
    hold_imag = (turn_imag * real_rate - (turn_real - 1.0) * frequency) / denominator
    push_real = jnp.einsum("sgh,gph->sgp", driven, input_map[0], precision=highest)
    push_imag = jnp.einsum("sgh,gph->sgp", driven, input_map[1], precision=highest)
    enter_real = push_real * hold_real - push_imag * hold_imag
    enter_imag = push_real * hold_imag + push_imag * hold_real
    old_real = prior_state[0].reshape(sequences, groups, -1)
    old_imag = prior_state[1].reshape(sequences, groups, -1)
    fresh_real = turn_real * old_real - turn_imag * old_imag + enter_real
    fresh_imag = turn_real * old_imag + turn_imag * old_real + enter_imag
    readout = jnp.einsum("ghp,sgp->sgh", output_map[0], fresh_real, precision=highest)
    readout = readout - jnp.einsum("ghp,sgp->sgh", output_map[1], fresh_imag, precision=highest)
    readout = readout.reshape(sequences, -1) + skip_gain * drive_rows.astype(jnp.float32)
    fresh = jnp.stack([fresh_real.reshape(sequences, -1), fresh_imag.reshape(sequences, -1)])
    return (readout, fresh)


def exchanged_experts(second_normed, routes, route_weights, expert_gate, expert_up, expert_down):
    experts = lax.axis_size("ep")
    seq_rows, top_count = routes.shape
    slot_cap = min(seq_rows, max(2, 3 * seq_rows * top_count // (2 * experts)))
    flat_routes = routes.reshape(-1)
    one_hot = (flat_routes[:, None] == jnp.arange(experts, dtype=jnp.int32)[None, :]).astype(
        jnp.int32
    )
    ranked = jnp.sum((jnp.cumsum(one_hot, axis=0) - one_hot) * one_hot, axis=1)
    slot_index = flat_routes * slot_cap + ranked
    placed = slot_index[:, None] == jnp.arange(experts * slot_cap, dtype=jnp.int32)[None, :]
    placed_rows = jnp.any(placed.reshape(seq_rows, top_count, experts * slot_cap), axis=1).astype(
        jnp.bfloat16
    )
    outgoing = lax.dot_general(
        placed_rows, second_normed, (((0,), (0,)), ((), ())), preferred_element_type=jnp.float32
    ).astype(jnp.bfloat16)
    outgoing = outgoing.reshape(experts, slot_cap, -1)
    arrived = lax.all_to_all(outgoing, "ep", split_axis=0, concat_axis=0, tiled=True)
    sources, count_items, full_width = arrived.shape
    expert_rows = arrived.reshape(sources * count_items, full_width)
    gate_val = jnp.dot(expert_rows, expert_gate[0], preferred_element_type=jnp.float32)
    up_val = jnp.dot(expert_rows, expert_up[0], preferred_element_type=jnp.float32)
    hidden = (jax.nn.silu(gate_val) * up_val).astype(jnp.bfloat16)
    piece = jnp.dot(hidden, expert_down[0], preferred_element_type=jnp.float32)
    summed = lax.psum_scatter(
        piece.reshape(sources, count_items, full_width).astype(jnp.bfloat16),
        "tp",
        scatter_dimension=2,
        tiled=True,
    )
    returned = lax.all_to_all(summed, "ep", split_axis=0, concat_axis=0, tiled=True)
    flat_back = returned.reshape(experts * slot_cap, -1)
    picked = (
        jnp.take(flat_back, slot_index, axis=0).reshape(seq_rows, top_count, -1).astype(jnp.float32)
    )
    routed = jnp.einsum("sk,skd->sd", route_weights, picked)
    return routed


def gathered_experts(second_normed, routes, route_weights, expert_gate, expert_up, expert_down):
    all_routes = lax.all_gather(routes, "ep", axis=0, tiled=True)
    all_weights = lax.all_gather(route_weights, "ep", axis=0, tiled=True)
    here = all_routes == lax.axis_index("ep")
    weight = jnp.sum(jnp.where(here, all_weights, 0.0), axis=1)
    rows = lax.all_gather(second_normed, "ep", axis=0, tiled=True)
    gate_val = jnp.dot(rows, expert_gate[0], preferred_element_type=jnp.float32)
    up_val = jnp.dot(rows, expert_up[0], preferred_element_type=jnp.float32)
    hidden = (jax.nn.silu(gate_val) * up_val).astype(jnp.bfloat16)
    piece = jnp.dot(hidden, expert_down[0], preferred_element_type=jnp.float32)
    summed = lax.psum_scatter(piece.astype(jnp.bfloat16), "tp", scatter_dimension=1, tiled=True)
    weighted = (weight[:, None] * summed.astype(jnp.float32)).astype(jnp.bfloat16)
    return lax.psum_scatter(weighted, "ep", scatter_dimension=0, tiled=True).astype(jnp.float32)


def body(
    tokens,
    prior_state,
    mix_gain,
    in_weight,
    decay_rate,
    frequency,
    log_step,
    input_map,
    output_map,
    skip_gain,
    out_weight,
    channel_gain,
    expert_gate,
    expert_up,
    expert_down,
    shared_gate,
    shared_up,
    shared_down,
    routes,
    route_weights,
):
    normed = root_scale(tokens, mix_gain)
    drive_rows = jnp.dot(normed, in_weight, preferred_element_type=jnp.float32).astype(jnp.bfloat16)
    readout, new_state = state_update(
        drive_rows, prior_state, decay_rate, frequency, log_step, input_map, output_map, skip_gain
    )
    activated = jax.nn.gelu(readout).astype(jnp.bfloat16)
    partial_value = jnp.dot(activated, out_weight, preferred_element_type=jnp.float32)
    mixer_out = lax.psum(partial_value.astype(jnp.bfloat16), "tp").astype(jnp.float32)
    middle = (tokens.astype(jnp.float32) + mixer_out).astype(jnp.bfloat16)
    second_normed = root_scale(middle, channel_gain)
    shared_gval = jnp.dot(second_normed, shared_gate, preferred_element_type=jnp.float32)
    shared_uval = jnp.dot(second_normed, shared_up, preferred_element_type=jnp.float32)
    shared_hidden = (jax.nn.silu(shared_gval) * shared_uval).astype(jnp.bfloat16)
    shared_piece = jnp.dot(shared_hidden, shared_down, preferred_element_type=jnp.float32)
    shared_out = lax.psum_scatter(
        shared_piece.astype(jnp.bfloat16), "tp", scatter_dimension=1, tiled=True
    ).astype(jnp.float32)
    experts = lax.axis_size("ep")
    half_cols = second_normed.shape[1] // lax.axis_size("tp")
    if experts <= 16:
        routed = gathered_experts(
            second_normed, routes, route_weights, expert_gate, expert_up, expert_down
        )
    else:
        routed = exchanged_experts(
            second_normed, routes, route_weights, expert_gate, expert_up, expert_down
        )
    own_middle = lax.dynamic_slice_in_dim(middle, lax.axis_index("tp") * half_cols, half_cols, 1)
    layer_out = (own_middle.astype(jnp.float32) + routed + shared_out).astype(jnp.bfloat16)
    return (layer_out, new_state)


def solution(mesh):
    in_specs = (
        P(("grp", "ep"), None),
        P(None, ("grp", "ep"), "tp"),
        P(),
        P(None, "tp"),
        P("tp", None),
        P("tp", None),
        P("tp"),
        P(None, "tp", None, None),
        P(None, "tp", None, None),
        P("tp"),
        P("tp", None),
        P(),
        P("ep", None, "tp"),
        P("ep", None, "tp"),
        P("ep", "tp", None),
        P(None, "tp"),
        P(None, "tp"),
        P("tp", None),
        P(("grp", "ep"), None),
        P(("grp", "ep"), None),
    )
    out_specs = (P(("grp", "ep"), "tp"), P(None, ("grp", "ep"), "tp"))
    return jax.shard_map(body, mesh=mesh, in_specs=in_specs, out_specs=out_specs, check_vma=False)
```

```python
import functools
import jax
import jax.numpy as jnp
from jax import lax
from jax.experimental import pallas as pl
from jax.experimental.pallas import tpu as pltpu
from jax.sharding import PartitionSpec as P

norm_eps = 1e-06
highest = lax.Precision.HIGHEST
MESH = pl.DeviceIdType.MESH


def root_scale(activations, scale_gain):
    values = activations.astype(jnp.float32)
    factor = lax.rsqrt(jnp.mean(values * values, axis=-1, keepdims=True) + norm_eps)
    return (values * factor * scale_gain).astype(jnp.bfloat16)


def state_update(
    drive_rows, prior_state, decay_rate, frequency, log_step, input_map, output_map, skip_gain
):
    sequences = drive_rows.shape[0]
    groups = decay_rate.shape[0]
    driven = drive_rows.astype(jnp.float32).reshape(sequences, groups, -1)
    step_size = jnp.exp(log_step)[:, None]
    real_rate = -decay_rate
    magnitude = jnp.exp(real_rate * step_size)
    turn_real = magnitude * jnp.cos(frequency * step_size)
    turn_imag = magnitude * jnp.sin(frequency * step_size)
    denominator = real_rate * real_rate + frequency * frequency
    hold_real = ((turn_real - 1.0) * real_rate + turn_imag * frequency) / denominator
    hold_imag = (turn_imag * real_rate - (turn_real - 1.0) * frequency) / denominator
    push_real = jnp.einsum("sgh,gph->sgp", driven, input_map[0], precision=highest)
    push_imag = jnp.einsum("sgh,gph->sgp", driven, input_map[1], precision=highest)
    enter_real = push_real * hold_real - push_imag * hold_imag
    enter_imag = push_real * hold_imag + push_imag * hold_real
    old_real = prior_state[0].reshape(sequences, groups, -1)
    old_imag = prior_state[1].reshape(sequences, groups, -1)
    fresh_real = turn_real * old_real - turn_imag * old_imag + enter_real
    fresh_imag = turn_real * old_imag + turn_imag * old_real + enter_imag
    readout = jnp.einsum("ghp,sgp->sgh", output_map[0], fresh_real, precision=highest)
    readout = readout - jnp.einsum("ghp,sgp->sgh", output_map[1], fresh_imag, precision=highest)
    readout = readout.reshape(sequences, -1) + skip_gain * drive_rows.astype(jnp.float32)
    fresh = jnp.stack([fresh_real.reshape(sequences, -1), fresh_imag.reshape(sequences, -1)])
    return (readout, fresh)


def exchanged_experts(second_normed, routes, route_weights, expert_gate, expert_up, expert_down):
    experts = lax.axis_size("ep")
    seq_rows, top_count = routes.shape
    slot_cap = min(seq_rows, max(2, 3 * seq_rows * top_count // (2 * experts)))
    flat_routes = routes.reshape(-1)
    one_hot = (flat_routes[:, None] == jnp.arange(experts, dtype=jnp.int32)[None, :]).astype(
        jnp.int32
    )
    ranked = jnp.sum((jnp.cumsum(one_hot, axis=0) - one_hot) * one_hot, axis=1)
    slot_index = flat_routes * slot_cap + ranked
    placed = slot_index[:, None] == jnp.arange(experts * slot_cap, dtype=jnp.int32)[None, :]
    placed_rows = jnp.any(placed.reshape(seq_rows, top_count, experts * slot_cap), axis=1).astype(
        jnp.bfloat16
    )
    outgoing = lax.dot_general(
        placed_rows, second_normed, (((0,), (0,)), ((), ())), preferred_element_type=jnp.float32
    ).astype(jnp.bfloat16)
    outgoing = outgoing.reshape(experts, slot_cap, -1)
    arrived = lax.all_to_all(outgoing, "ep", split_axis=0, concat_axis=0, tiled=True)
    sources, count_items, full_width = arrived.shape
    expert_rows = arrived.reshape(sources * count_items, full_width)
    gate_val = jnp.dot(expert_rows, expert_gate[0], preferred_element_type=jnp.float32)
    up_val = jnp.dot(expert_rows, expert_up[0], preferred_element_type=jnp.float32)
    hidden = (jax.nn.silu(gate_val) * up_val).astype(jnp.bfloat16)
    piece = jnp.dot(hidden, expert_down[0], preferred_element_type=jnp.float32)
    summed = lax.psum_scatter(
        piece.reshape(sources, count_items, full_width).astype(jnp.bfloat16),
        "tp",
        scatter_dimension=2,
        tiled=True,
    )
    returned = lax.all_to_all(summed, "ep", split_axis=0, concat_axis=0, tiled=True)
    flat_back = returned.reshape(experts * slot_cap, -1)
    picked = (
        jnp.take(flat_back, slot_index, axis=0).reshape(seq_rows, top_count, -1).astype(jnp.float32)
    )
    routed = jnp.einsum("sk,skd->sd", route_weights, picked)
    return routed


def near_first(extent):
    return [sorted(range(extent), key=lambda other: (abs(other - at), other)) for at in range(extent)]


def looked_up(table, position):
    found = jnp.int32(0)
    for at, entry in enumerate(table):
        found = jnp.where(position == at, jnp.int32(entry), found)
    return found


def expert_kernel(
    grid_shape, pieces,
    own, middle, weights, gate_in, up_in, down_in, sgate_in, sup_in, sdown_in,
    out,
    rows_all, back, from_twin, from_side, from_far, weight_all,
    gate, up, down, sgate, sup, sdown, hidden, shared, total,
    load_sem, row_recv, own_z_send, fwd_z_send, fwd_x_send, fwd_twin_send,
    w_send, w_recv, twin_send, twin_recv, side_send, side_recv, far_send, far_recv,
):
    zs, xs, cs = grid_shape
    count = zs * xs * cs
    me = lax.axis_index("ep")
    core = lax.rem(me, cs)
    col = lax.rem(me // cs, xs)
    level = me // (cs * xs)
    rows, width = own.shape
    span = rows // pieces
    hid = gate.shape[1]

    def device(z, x, c):
        return (z * xs + x) * cs + c

    twin = device(level, col, 1 - core)
    side = device(level, 1 - col, core)
    order = [looked_up([row[j] for row in near_first(zs)], level) for j in range(zs)]

    def part(base, h):
        return pl.ds(pl.multiple_of(base * rows + h * span, 16), span)

    loads = [
        pltpu.make_async_copy(src, dst, load_sem.at[n])
        for n, (src, dst) in enumerate(
            ((sgate_in, sgate), (sup_in, sup), (sdown_in, sdown),
             (gate_in.at[0], gate), (up_in.at[0], up), (down_in.at[0], down))
        )
    ]
    for load in loads:
        load.start()

    barrier = pltpu.get_barrier_semaphore()
    for step in range(1, count):
        pl.semaphore_signal(
            barrier, inc=1, device_id={"ep": lax.rem(me + step, count)}, device_id_type=MESH
        )
    pl.semaphore_wait(barrier, count - 1)

    def remote(src, dst, send, recv, target):
        return pltpu.make_async_remote_copy(
            src_ref=src, dst_ref=dst, send_sem=send, recv_sem=recv,
            device_id={"ep": target}, device_id_type=MESH,
        )

    sent = []

    def push(src, dst, send, recv, target):
        copy = remote(src, dst, send, recv, target)
        copy.start()
        sent.append(copy)

    def row_copy(src_ref, src_rows, origin, h, send, target):
        return remote(
            src_ref.at[src_rows], rows_all.at[part(origin, h)], send, row_recv.at[origin, h], target
        )

    for h in range(pieces):
        piece = pl.ds(h * span, span)

        @pl.when(level > 0)
        def _():
            row_copy(own, piece, me, h, own_z_send.at[0, h], device(level - 1, col, core)).start()

        @pl.when(level < zs - 1)
        def _():
            row_copy(own, piece, me, h, own_z_send.at[1, h], device(level + 1, col, core)).start()

        for send, target in ((fwd_x_send.at[0, h], side), (fwd_twin_send.at[0, h], twin)):
            copy = row_copy(own, piece, me, h, send, target)
            copy.start()
            sent.append(copy)

    for step in range(1, count):
        other = lax.rem(me + step, count)
        push(
            weights.at[other], weight_all.at[me], w_send.at[step], w_recv.at[count - step], other
        )
    rows_all[part(me, 0), :] = own[pl.ds(0, span), :]
    for h in range(1, pieces):
        rows_all[part(me, h), :] = own[pl.ds(h * span, span), :]
    weight_all[me] = weights[me]

    def arrived(origin, h):
        row_copy(own, pl.ds(h * span, span), origin, h, own_z_send.at[0, h], twin).wait_recv()

    def feed(source, take, gate_w, up_w, down_w, finish):
        def first(n, carry):
            cols = pl.ds(pl.multiple_of(n * 256, 256), 256)
            data = source()
            g = jnp.dot(data, gate_w[:, cols], preferred_element_type=jnp.float32)
            u = jnp.dot(data, up_w[:, cols], preferred_element_type=jnp.float32)
            hidden[pl.ds(0, take), cols] = (jax.nn.silu(g) * u).astype(jnp.bfloat16)
            return carry

        lax.fori_loop(0, hid // 256, first, 0)

        def second(n, carry):
            cols = pl.ds(pl.multiple_of(n * 512, 512), 512)
            piece = jnp.dot(
                hidden[pl.ds(0, take), :], down_w[:, cols], preferred_element_type=jnp.float32
            )
            finish(cols, piece.astype(jnp.bfloat16))
            return carry

        lax.fori_loop(0, width // 512, second, 0)

    def chip(label, z, x):
        base = device(z, x, 0)
        block = pl.ds(pl.multiple_of(base * rows, 16), cs * rows)
        scales = []
        for c in range(cs):
            line = jnp.broadcast_to(weight_all[base + c], (128, 128))
            scales.append(jnp.transpose(line)[:rows])
        scale = jnp.concatenate(scales, axis=0)
        scale = jnp.concatenate([scale] * 4, axis=1)

        def finish(cols, piece):
            back[block, cols] = (piece.astype(jnp.float32) * scale).astype(jnp.bfloat16)

        feed(lambda: rows_all[block, :], cs * rows, gate, up, down, finish)
        push(
            back.at[part_all(device(z, x, 1 - core))],
            from_twin.at[label],
            twin_send.at[label],
            twin_recv.at[label],
            twin,
        )

    def part_all(origin):
        return pl.ds(pl.multiple_of(origin * rows, 16), rows)

    for load in loads[:3]:
        load.wait()

    def keep(cols, piece):
        shared[:, cols] = piece

    feed(lambda: own[...], rows, sgate, sup, sdown, keep)
    for load in loads[3:]:
        load.wait()
    for step in range(1, count):
        remote(
            weights.at[me], weight_all.at[lax.rem(me + step, count)],
            w_send.at[step], w_recv.at[step], twin,
        ).wait_recv()

    def pair_in(z, x):
        for h in range(pieces):
            arrived(device(z, x, 1 - core), h)

    pair_in(level, col)
    chip(0, level, col)
    for j in range(1, zs + 1):
        if j < zs:
            origin_z = order[j]
            origin = device(origin_z, col, core)
            for h in range(pieces):
                arrived(origin, h)
                onward = jnp.where(origin_z < level, level + 1, level - 1)

                @pl.when((onward >= 0) & (onward < zs))
                def _():
                    row_copy(
                        rows_all, part(origin, h), origin, h, fwd_z_send.at[j, h],
                        device(onward, col, core),
                    ).start()

                for send, target in ((fwd_x_send.at[j, h], side), (fwd_twin_send.at[j, h], twin)):
                    copy = row_copy(rows_all, part(origin, h), origin, h, send, target)
                    copy.start()
                    sent.append(copy)
        across = device(order[j - 1], 1 - col, core)
        for h in range(pieces):
            arrived(across, h)
            copy = row_copy(
                rows_all, part(across, h), across, h, fwd_twin_send.at[zs + j - 1, h], twin
            )
            copy.start()
            sent.append(copy)
        if j < zs:
            pair_in(order[j], col)
            chip(j, order[j], col)
        pair_in(order[j - 1], 1 - col)
        chip(zs + j - 1, order[j - 1], 1 - col)

    def twin_in(label):
        remote(
            from_twin.at[label], from_twin.at[label], twin_send.at[label], twin_recv.at[label], twin
        ).wait_recv()

    def added(first, others, store):
        def strip(n, carry):
            at = pl.multiple_of(n * 16, 16)
            value = first(at).astype(jnp.float32)
            for other in others:
                value = value + other(at).astype(jnp.float32)
            store(at, value)
            return carry

        lax.fori_loop(0, span // 16, strip, 0)

    def back_at(origin, h):
        return lambda at: back[pl.ds(pl.multiple_of(origin * rows + h * span + at, 16), 16), :]

    def slot_at(ref, slot, h):
        return lambda at: ref[slot, pl.ds(pl.multiple_of(h * span + at, 16), 16), :]

    def to_back(origin, h):
        def store(at, value):
            back[pl.ds(pl.multiple_of(origin * rows + h * span + at, 16), 16), :] = value.astype(
                jnp.bfloat16
            )

        return store

    for j in reversed(range(zs)):
        twin_in(zs + j)
        origin = device(order[j], 1 - col, core)
        for h in range(pieces):
            added(back_at(origin, h), [slot_at(from_twin, zs + j, h)], to_back(origin, h))
            push(
                back.at[part(origin, h)], from_side.at[j, pl.ds(h * span, span)],
                side_send.at[j, h], side_recv.at[j, h], side,
            )

    def side_in(j, h):
        view = from_side.at[j, pl.ds(h * span, span)]
        remote(view, view, side_send.at[j, h], side_recv.at[j, h], side).wait_recv()

    def far_in(slot, h):
        view = from_far.at[slot, pl.ds(h * span, span)]
        remote(view, view, far_send.at[0, h], far_recv.at[slot, h], side).wait_recv()

    for j in reversed(range(1, zs)):
        twin_in(j)
        goal = order[j]
        origin = device(goal, col, core)
        nearer = jnp.where(goal < level, level - 1, level + 1)
        behind = jnp.where(goal < level, level + 1, level - 1)
        slot = jnp.where((nearer == goal) & (goal > level), zs, goal)
        for h in range(pieces):
            side_in(j, h)
            terms = [slot_at(from_twin, j, h), slot_at(from_side, j, h)]

            @pl.when((behind >= 0) & (behind < zs))
            def _():
                far_in(goal, h)
                added(
                    back_at(origin, h), terms + [slot_at(from_far, goal, h)], to_back(origin, h)
                )

            @pl.when((behind < 0) | (behind >= zs))
            def _():
                added(back_at(origin, h), terms, to_back(origin, h))

            push(
                back.at[part(origin, h)], from_far.at[slot, pl.ds(h * span, span)],
                far_send.at[j, h], far_recv.at[slot, h], device(nearer, col, core),
            )
    twin_in(0)
    for h in range(pieces):
        side_in(0, h)

        def to_total(at, value):
            total[pl.ds(pl.multiple_of(h * span + at, 16), 16), :] = value

        def total_at(at):
            return total[pl.ds(pl.multiple_of(h * span + at, 16), 16), :]

        added(back_at(me, h), [slot_at(from_twin, 0, h), slot_at(from_side, 0, h)], to_total)

        @pl.when(level > 0)
        def _():
            far_in(zs, h)
            added(total_at, [slot_at(from_far, zs, h)], to_total)

        @pl.when(level < zs - 1)
        def _():
            far_in(level, h)
            added(total_at, [slot_at(from_far, level, h)], to_total)

        def plain(ref):
            return lambda at: ref[pl.ds(pl.multiple_of(h * span + at, 16), 16), :]

        def to_out(at, value):
            out[pl.ds(pl.multiple_of(h * span + at, 16), 16), :] = value.astype(jnp.bfloat16)

        added(plain(middle), [total_at, plain(shared)], to_out)

    for copy in sent:
        copy.wait_send()
    for h in range(pieces):
        piece = pl.ds(h * span, span)

        @pl.when(level > 0)
        def _():
            row_copy(own, piece, me, h, own_z_send.at[0, h], twin).wait_send()

        @pl.when(level < zs - 1)
        def _():
            row_copy(own, piece, me, h, own_z_send.at[1, h], twin).wait_send()

        for j in range(1, zs):
            onward = jnp.where(order[j] < level, level + 1, level - 1)

            @pl.when((onward >= 0) & (onward < zs))
            def _():
                row_copy(own, piece, me, h, fwd_z_send.at[j, h], twin).wait_send()


def expert_stage(
    second_normed, middle, routes, route_weights,
    expert_gate, expert_up, expert_down, shared_gate, shared_up, shared_down,
):
    experts = lax.axis_size("ep")
    grid_shape = (experts // 4, 2, 2)
    zs = grid_shape[0]
    rows, width = second_normed.shape
    hid = expert_gate.shape[2]
    pieces = 2 if rows % 32 == 0 else 1
    chosen = routes[None, :, :] == jnp.arange(experts, dtype=jnp.int32)[:, None, None]
    weights = jnp.sum(jnp.where(chosen, route_weights[None], 0.0), axis=2)
    weights = jnp.pad(weights, ((0, 0), (0, 128 - rows)))[:, None, :]
    vmem = pl.BlockSpec(memory_space=pltpu.VMEM)
    hbm = pl.BlockSpec(memory_space=pl.ANY)
    dma = pltpu.SemaphoreType.DMA
    half = jnp.bfloat16
    return pl.pallas_call(
        functools.partial(expert_kernel, grid_shape, pieces),
        out_shape=jax.ShapeDtypeStruct((rows, width), half),
        in_specs=[vmem] * 3 + [hbm] * 6,
        out_specs=vmem,
        scratch_shapes=[
            pltpu.VMEM((experts * rows, width), half),
            pltpu.VMEM((experts * rows, width), half),
            pltpu.VMEM((2 * zs, rows, width), half),
            pltpu.VMEM((zs, rows, width), half),
            pltpu.VMEM((zs + 1, rows, width), half),
            pltpu.VMEM((experts, 1, 128), jnp.float32),
            pltpu.VMEM((width, hid), half),
            pltpu.VMEM((width, hid), half),
            pltpu.VMEM((hid, width), half),
            pltpu.VMEM(shared_gate.shape, half),
            pltpu.VMEM(shared_up.shape, half),
            pltpu.VMEM(shared_down.shape, half),
            pltpu.VMEM((2 * rows, hid), half),
            pltpu.VMEM((rows, width), half),
            pltpu.VMEM((rows, width), jnp.float32),
            dma((6,)),
            dma((experts, pieces)),
            dma((2, pieces)),
            dma((zs, pieces)),
            dma((zs, pieces)),
            dma((2 * zs, pieces)),
            dma((experts,)),
            dma((experts,)),
            dma((2 * zs,)),
            dma((2 * zs,)),
            dma((zs, pieces)),
            dma((zs, pieces)),
            dma((zs, pieces)),
            dma((zs + 1, pieces)),
        ],
        compiler_params=pltpu.CompilerParams(
            collective_id=0, has_side_effects=True, vmem_limit_bytes=60 * 1024 * 1024
        ),
    )(
        second_normed, middle, weights,
        expert_gate, expert_up, expert_down, shared_gate, shared_up, shared_down,
    )


def body(
    tokens,
    prior_state,
    mix_gain,
    in_weight,
    decay_rate,
    frequency,
    log_step,
    input_map,
    output_map,
    skip_gain,
    out_weight,
    channel_gain,
    expert_gate,
    expert_up,
    expert_down,
    shared_gate,
    shared_up,
    shared_down,
    routes,
    route_weights,
):
    normed = root_scale(tokens, mix_gain)
    drive_rows = jnp.dot(normed, in_weight, preferred_element_type=jnp.float32).astype(jnp.bfloat16)
    readout, new_state = state_update(
        drive_rows, prior_state, decay_rate, frequency, log_step, input_map, output_map, skip_gain
    )
    activated = jax.nn.gelu(readout).astype(jnp.bfloat16)
    partial_value = jnp.dot(activated, out_weight, preferred_element_type=jnp.float32)
    mixer_out = lax.psum(partial_value.astype(jnp.bfloat16), "tp").astype(jnp.float32)
    middle = (tokens.astype(jnp.float32) + mixer_out).astype(jnp.bfloat16)
    second_normed = root_scale(middle, channel_gain)
    if lax.axis_size("tp") == 1 and lax.axis_size("ep") == 16:
        layer_out = expert_stage(
            second_normed, middle, routes, route_weights,
            expert_gate, expert_up, expert_down, shared_gate, shared_up, shared_down,
        )
        return (layer_out, new_state)
    shared_gval = jnp.dot(second_normed, shared_gate, preferred_element_type=jnp.float32)
    shared_uval = jnp.dot(second_normed, shared_up, preferred_element_type=jnp.float32)
    shared_hidden = (jax.nn.silu(shared_gval) * shared_uval).astype(jnp.bfloat16)
    shared_piece = jnp.dot(shared_hidden, shared_down, preferred_element_type=jnp.float32)
    shared_out = lax.psum_scatter(
        shared_piece.astype(jnp.bfloat16), "tp", scatter_dimension=1, tiled=True
    ).astype(jnp.float32)
    half_cols = second_normed.shape[1] // lax.axis_size("tp")
    routed = exchanged_experts(
        second_normed, routes, route_weights, expert_gate, expert_up, expert_down
    )
    own_middle = lax.dynamic_slice_in_dim(middle, lax.axis_index("tp") * half_cols, half_cols, 1)
    layer_out = (own_middle.astype(jnp.float32) + routed + shared_out).astype(jnp.bfloat16)
    return (layer_out, new_state)


def solution(mesh):
    in_specs = (
        P(("grp", "ep"), None),
        P(None, ("grp", "ep"), "tp"),
        P(),
        P(None, "tp"),
        P("tp", None),
        P("tp", None),
        P("tp"),
        P(None, "tp", None, None),
        P(None, "tp", None, None),
        P("tp"),
        P("tp", None),
        P(),
        P("ep", None, "tp"),
        P("ep", None, "tp"),
        P("ep", "tp", None),
        P(None, "tp"),
        P(None, "tp"),
        P("tp", None),
        P(("grp", "ep"), None),
        P(("grp", "ep"), None),
    )
    out_specs = (P(("grp", "ep"), "tp"), P(None, ("grp", "ep"), "tp"))
    return jax.shard_map(body, mesh=mesh, in_specs=in_specs, out_specs=out_specs, check_vma=False)
```

```python
import functools
import jax
import jax.numpy as jnp
from jax import lax
from jax.experimental import pallas as pl
from jax.experimental.pallas import tpu as pltpu
from jax.sharding import PartitionSpec as P

norm_eps = 1e-06
highest = lax.Precision.HIGHEST
MESH = pl.DeviceIdType.MESH


def root_scale(activations, scale_gain):
    values = activations.astype(jnp.float32)
    factor = lax.rsqrt(jnp.mean(values * values, axis=-1, keepdims=True) + norm_eps)
    return (values * factor * scale_gain).astype(jnp.bfloat16)


def state_update(
    drive_rows, prior_state, decay_rate, frequency, log_step, input_map, output_map, skip_gain
):
    sequences = drive_rows.shape[0]
    groups = decay_rate.shape[0]
    driven = drive_rows.astype(jnp.float32).reshape(sequences, groups, -1)
    step_size = jnp.exp(log_step)[:, None]
    real_rate = -decay_rate
    magnitude = jnp.exp(real_rate * step_size)
    turn_real = magnitude * jnp.cos(frequency * step_size)
    turn_imag = magnitude * jnp.sin(frequency * step_size)
    denominator = real_rate * real_rate + frequency * frequency
    hold_real = ((turn_real - 1.0) * real_rate + turn_imag * frequency) / denominator
    hold_imag = (turn_imag * real_rate - (turn_real - 1.0) * frequency) / denominator
    push_real = jnp.einsum("sgh,gph->sgp", driven, input_map[0], precision=highest)
    push_imag = jnp.einsum("sgh,gph->sgp", driven, input_map[1], precision=highest)
    enter_real = push_real * hold_real - push_imag * hold_imag
    enter_imag = push_real * hold_imag + push_imag * hold_real
    old_real = prior_state[0].reshape(sequences, groups, -1)
    old_imag = prior_state[1].reshape(sequences, groups, -1)
    fresh_real = turn_real * old_real - turn_imag * old_imag + enter_real
    fresh_imag = turn_real * old_imag + turn_imag * old_real + enter_imag
    readout = jnp.einsum("ghp,sgp->sgh", output_map[0], fresh_real, precision=highest)
    readout = readout - jnp.einsum("ghp,sgp->sgh", output_map[1], fresh_imag, precision=highest)
    readout = readout.reshape(sequences, -1) + skip_gain * drive_rows.astype(jnp.float32)
    fresh = jnp.stack([fresh_real.reshape(sequences, -1), fresh_imag.reshape(sequences, -1)])
    return (readout, fresh)


def exchanged_experts(second_normed, routes, route_weights, expert_gate, expert_up, expert_down):
    experts = lax.axis_size("ep")
    seq_rows, top_count = routes.shape
    slot_cap = min(seq_rows, max(2, 3 * seq_rows * top_count // (2 * experts)))
    flat_routes = routes.reshape(-1)
    one_hot = (flat_routes[:, None] == jnp.arange(experts, dtype=jnp.int32)[None, :]).astype(
        jnp.int32
    )
    ranked = jnp.sum((jnp.cumsum(one_hot, axis=0) - one_hot) * one_hot, axis=1)
    slot_index = flat_routes * slot_cap + ranked
    placed = slot_index[:, None] == jnp.arange(experts * slot_cap, dtype=jnp.int32)[None, :]
    placed_rows = jnp.any(placed.reshape(seq_rows, top_count, experts * slot_cap), axis=1).astype(
        jnp.bfloat16
    )
    outgoing = lax.dot_general(
        placed_rows, second_normed, (((0,), (0,)), ((), ())), preferred_element_type=jnp.float32
    ).astype(jnp.bfloat16)
    outgoing = outgoing.reshape(experts, slot_cap, -1)
    arrived = lax.all_to_all(outgoing, "ep", split_axis=0, concat_axis=0, tiled=True)
    sources, count_items, full_width = arrived.shape
    expert_rows = arrived.reshape(sources * count_items, full_width)
    gate_val = jnp.dot(expert_rows, expert_gate[0], preferred_element_type=jnp.float32)
    up_val = jnp.dot(expert_rows, expert_up[0], preferred_element_type=jnp.float32)
    hidden = (jax.nn.silu(gate_val) * up_val).astype(jnp.bfloat16)
    piece = jnp.dot(hidden, expert_down[0], preferred_element_type=jnp.float32)
    summed = lax.psum_scatter(
        piece.reshape(sources, count_items, full_width).astype(jnp.bfloat16),
        "tp",
        scatter_dimension=2,
        tiled=True,
    )
    returned = lax.all_to_all(summed, "ep", split_axis=0, concat_axis=0, tiled=True)
    flat_back = returned.reshape(experts * slot_cap, -1)
    picked = (
        jnp.take(flat_back, slot_index, axis=0).reshape(seq_rows, top_count, -1).astype(jnp.float32)
    )
    routed = jnp.einsum("sk,skd->sd", route_weights, picked)
    return routed


def near_first(extent):
    return [sorted(range(extent), key=lambda other: (abs(other - at), other)) for at in range(extent)]


def looked_up(table, position):
    found = jnp.int32(0)
    for at, entry in enumerate(table):
        found = jnp.where(position == at, jnp.int32(entry), found)
    return found


def expert_kernel(
    grid_shape, pieces,
    own, middle, weights, gate_in, up_in, down_in, sgate_in, sup_in, sdown_in,
    out,
    rows_all, back, from_twin, from_side, from_far, weight_all,
    gate, up, down, sgate, sup, sdown, hidden, shared, total,
    load_sem, row_recv, own_z_send, fwd_z_send, fwd_x_send, fwd_twin_send,
    w_send, w_recv, twin_send, twin_recv, side_send, side_recv, far_send, far_recv,
):
    zs, xs, cs = grid_shape
    count = zs * xs * cs
    me = lax.axis_index("ep")
    core = lax.rem(me, cs)
    col = lax.rem(me // cs, xs)
    level = me // (cs * xs)
    rows, width = own.shape
    span = rows // pieces
    hid = gate.shape[1]

    def device(z, x, c):
        return (z * xs + x) * cs + c

    twin = device(level, col, 1 - core)
    side = device(level, 1 - col, core)
    order = [looked_up([row[j] for row in near_first(zs)], level) for j in range(zs)]

    def part(base, h):
        return pl.ds(pl.multiple_of(base * rows + h * span, 16), span)

    loads = [
        pltpu.make_async_copy(src, dst, load_sem.at[n])
        for n, (src, dst) in enumerate(
            ((sgate_in, sgate), (sup_in, sup), (sdown_in, sdown),
             (gate_in.at[0], gate), (up_in.at[0], up), (down_in.at[0], down))
        )
    ]
    for load in loads:
        load.start()

    barrier = pltpu.get_barrier_semaphore()
    for step in range(1, count):
        pl.semaphore_signal(
            barrier, inc=1, device_id={"ep": lax.rem(me + step, count)}, device_id_type=MESH
        )
    pl.semaphore_wait(barrier, count - 1)

    def remote(src, dst, send, recv, target):
        return pltpu.make_async_remote_copy(
            src_ref=src, dst_ref=dst, send_sem=send, recv_sem=recv,
            device_id={"ep": target}, device_id_type=MESH,
        )

    sent = []

    def push(src, dst, send, recv, target):
        copy = remote(src, dst, send, recv, target)
        copy.start()
        sent.append(copy)

    def row_copy(src_ref, src_rows, origin, h, send, target):
        return remote(
            src_ref.at[src_rows], rows_all.at[part(origin, h)], send, row_recv.at[origin, h], target
        )

    for h in range(pieces):
        piece = pl.ds(h * span, span)

        @pl.when(level > 0)
        def _():
            row_copy(own, piece, me, h, own_z_send.at[0, h], device(level - 1, col, core)).start()

        @pl.when(level < zs - 1)
        def _():
            row_copy(own, piece, me, h, own_z_send.at[1, h], device(level + 1, col, core)).start()

        for send, target in ((fwd_x_send.at[0, h], side), (fwd_twin_send.at[0, h], twin)):
            copy = row_copy(own, piece, me, h, send, target)
            copy.start()
            sent.append(copy)

    for step in range(1, count):
        other = lax.rem(me + step, count)
        push(
            weights.at[other], weight_all.at[me], w_send.at[step], w_recv.at[count - step], other
        )
    rows_all[part(me, 0), :] = own[pl.ds(0, span), :]
    for h in range(1, pieces):
        rows_all[part(me, h), :] = own[pl.ds(h * span, span), :]
    weight_all[me] = weights[me]

    def arrived(origin, h):
        row_copy(own, pl.ds(h * span, span), origin, h, own_z_send.at[0, h], twin).wait_recv()

    def feed(source, take, gate_w, up_w, down_w, finish):
        def first(n, carry):
            cols = pl.ds(pl.multiple_of(n * 256, 256), 256)
            data = source()
            g = jnp.dot(data, gate_w[:, cols], preferred_element_type=jnp.float32)
            u = jnp.dot(data, up_w[:, cols], preferred_element_type=jnp.float32)
            hidden[pl.ds(0, take), cols] = (jax.nn.silu(g) * u).astype(jnp.bfloat16)
            return carry

        lax.fori_loop(0, hid // 256, first, 0)

        def second(n, carry):
            cols = pl.ds(pl.multiple_of(n * 512, 512), 512)
            piece = jnp.dot(
                hidden[pl.ds(0, take), :], down_w[:, cols], preferred_element_type=jnp.float32
            )
            finish(cols, piece.astype(jnp.bfloat16))
            return carry

        lax.fori_loop(0, width // 512, second, 0)

    def chip(label, z, x):
        base = device(z, x, 0)
        block = pl.ds(pl.multiple_of(base * rows, 16), cs * rows)
        scales = []
        for c in range(cs):
            line = jnp.broadcast_to(weight_all[base + c], (128, 128))
            scales.append(jnp.transpose(line)[:rows])
        scale = jnp.concatenate(scales, axis=0)
        scale = jnp.concatenate([scale] * 4, axis=1)

        def finish(cols, piece):
            back[block, cols] = (piece.astype(jnp.float32) * scale).astype(jnp.bfloat16)

        feed(lambda: rows_all[block, :], cs * rows, gate, up, down, finish)
        push(
            back.at[part_all(device(z, x, 1 - core))],
            from_twin.at[label],
            twin_send.at[label],
            twin_recv.at[label],
            twin,
        )

    def part_all(origin):
        return pl.ds(pl.multiple_of(origin * rows, 16), rows)

    for load in loads[:3]:
        load.wait()

    def keep(cols, piece):
        shared[:, cols] = piece

    feed(lambda: own[...], rows, sgate, sup, sdown, keep)
    for load in loads[3:]:
        load.wait()
    for step in range(1, count):
        remote(
            weights.at[me], weight_all.at[lax.rem(me + step, count)],
            w_send.at[step], w_recv.at[step], twin,
        ).wait_recv()

    def pair_in(z, x):
        for h in range(pieces):
            arrived(device(z, x, 1 - core), h)

    pair_in(level, col)
    chip(0, level, col)
    for j in range(1, zs + 1):
        if j < zs:
            origin_z = order[j]
            origin = device(origin_z, col, core)
            for h in range(pieces):
                arrived(origin, h)
                onward = jnp.where(origin_z < level, level + 1, level - 1)

                @pl.when((onward >= 0) & (onward < zs))
                def _():
                    row_copy(
                        rows_all, part(origin, h), origin, h, fwd_z_send.at[j, h],
                        device(onward, col, core),
                    ).start()

                for send, target in ((fwd_x_send.at[j, h], side), (fwd_twin_send.at[j, h], twin)):
                    copy = row_copy(rows_all, part(origin, h), origin, h, send, target)
                    copy.start()
                    sent.append(copy)
        across = device(order[j - 1], 1 - col, core)
        for h in range(pieces):
            arrived(across, h)
            copy = row_copy(
                rows_all, part(across, h), across, h, fwd_twin_send.at[zs + j - 1, h], twin
            )
            copy.start()
            sent.append(copy)
        if j < zs:
            pair_in(order[j], col)
            chip(j, order[j], col)
        pair_in(order[j - 1], 1 - col)
        chip(zs + j - 1, order[j - 1], 1 - col)

    def twin_in(label):
        remote(
            from_twin.at[label], from_twin.at[label], twin_send.at[label], twin_recv.at[label], twin
        ).wait_recv()

    def added(first, others, store):
        def strip(n, carry):
            at = pl.multiple_of(n * 16, 16)
            value = first(at).astype(jnp.float32)
            for other in others:
                value = value + other(at).astype(jnp.float32)
            store(at, value)
            return carry

        lax.fori_loop(0, span // 16, strip, 0)

    def back_at(origin, h):
        return lambda at: back[pl.ds(pl.multiple_of(origin * rows + h * span + at, 16), 16), :]

    def slot_at(ref, slot, h):
        return lambda at: ref[slot, pl.ds(pl.multiple_of(h * span + at, 16), 16), :]

    def to_back(origin, h):
        def store(at, value):
            back[pl.ds(pl.multiple_of(origin * rows + h * span + at, 16), 16), :] = value.astype(
                jnp.bfloat16
            )

        return store

    for j in reversed(range(zs)):
        twin_in(zs + j)
        origin = device(order[j], 1 - col, core)
        for h in range(pieces):
            added(back_at(origin, h), [slot_at(from_twin, zs + j, h)], to_back(origin, h))
            push(
                back.at[part(origin, h)], from_side.at[j, pl.ds(h * span, span)],
                side_send.at[j, h], side_recv.at[j, h], side,
            )

    def side_in(j, h):
        view = from_side.at[j, pl.ds(h * span, span)]
        remote(view, view, side_send.at[j, h], side_recv.at[j, h], side).wait_recv()

    def far_in(slot, h):
        view = from_far.at[slot, pl.ds(h * span, span)]
        remote(view, view, far_send.at[0, h], far_recv.at[slot, h], side).wait_recv()

    for j in reversed(range(1, zs)):
        twin_in(j)
        goal = order[j]
        origin = device(goal, col, core)
        nearer = jnp.where(goal < level, level - 1, level + 1)
        behind = jnp.where(goal < level, level + 1, level - 1)
        slot = jnp.where((nearer == goal) & (goal > level), zs, goal)
        for h in range(pieces):
            side_in(j, h)
            terms = [slot_at(from_twin, j, h), slot_at(from_side, j, h)]

            @pl.when((behind >= 0) & (behind < zs))
            def _():
                far_in(goal, h)
                added(
                    back_at(origin, h), terms + [slot_at(from_far, goal, h)], to_back(origin, h)
                )

            @pl.when((behind < 0) | (behind >= zs))
            def _():
                added(back_at(origin, h), terms, to_back(origin, h))

            push(
                back.at[part(origin, h)], from_far.at[slot, pl.ds(h * span, span)],
                far_send.at[j, h], far_recv.at[slot, h], device(nearer, col, core),
            )
    twin_in(0)
    for h in range(pieces):
        side_in(0, h)

        def to_total(at, value):
            total[pl.ds(pl.multiple_of(h * span + at, 16), 16), :] = value

        def total_at(at):
            return total[pl.ds(pl.multiple_of(h * span + at, 16), 16), :]

        added(back_at(me, h), [slot_at(from_twin, 0, h), slot_at(from_side, 0, h)], to_total)

        @pl.when(level > 0)
        def _():
            far_in(zs, h)
            added(total_at, [slot_at(from_far, zs, h)], to_total)

        @pl.when(level < zs - 1)
        def _():
            far_in(level, h)
            added(total_at, [slot_at(from_far, level, h)], to_total)

        def plain(ref):
            return lambda at: ref[pl.ds(pl.multiple_of(h * span + at, 16), 16), :]

        def to_out(at, value):
            out[pl.ds(pl.multiple_of(h * span + at, 16), 16), :] = value.astype(jnp.bfloat16)

        added(plain(middle), [total_at, plain(shared)], to_out)

    for copy in sent:
        copy.wait_send()
    for h in range(pieces):
        piece = pl.ds(h * span, span)

        @pl.when(level > 0)
        def _():
            row_copy(own, piece, me, h, own_z_send.at[0, h], twin).wait_send()

        @pl.when(level < zs - 1)
        def _():
            row_copy(own, piece, me, h, own_z_send.at[1, h], twin).wait_send()

        for j in range(1, zs):
            onward = jnp.where(order[j] < level, level + 1, level - 1)

            @pl.when((onward >= 0) & (onward < zs))
            def _():
                row_copy(own, piece, me, h, fwd_z_send.at[j, h], twin).wait_send()


def expert_stage(
    second_normed, middle, routes, route_weights,
    expert_gate, expert_up, expert_down, shared_gate, shared_up, shared_down,
):
    experts = lax.axis_size("ep")
    grid_shape = (experts // 4, 2, 2)
    zs = grid_shape[0]
    rows, width = second_normed.shape
    hid = expert_gate.shape[2]
    pieces = 2 if rows % 32 == 0 else 1
    chosen = routes[None, :, :] == jnp.arange(experts, dtype=jnp.int32)[:, None, None]
    weights = jnp.sum(jnp.where(chosen, route_weights[None], 0.0), axis=2)
    weights = jnp.pad(weights, ((0, 0), (0, 128 - rows)))[:, None, :]
    vmem = pl.BlockSpec(memory_space=pltpu.VMEM)
    hbm = pl.BlockSpec(memory_space=pl.ANY)
    dma = pltpu.SemaphoreType.DMA
    half = jnp.bfloat16
    return pl.pallas_call(
        functools.partial(expert_kernel, grid_shape, pieces),
        out_shape=jax.ShapeDtypeStruct((rows, width), half),
        in_specs=[vmem] * 3 + [hbm] * 6,
        out_specs=vmem,
        scratch_shapes=[
            pltpu.VMEM((experts * rows, width), half),
            pltpu.VMEM((experts * rows, width), half),
            pltpu.VMEM((2 * zs, rows, width), half),
            pltpu.VMEM((zs, rows, width), half),
            pltpu.VMEM((zs + 1, rows, width), half),
            pltpu.VMEM((experts, 1, 128), jnp.float32),
            pltpu.VMEM((width, hid), half),
            pltpu.VMEM((width, hid), half),
            pltpu.VMEM((hid, width), half),
            pltpu.VMEM(shared_gate.shape, half),
            pltpu.VMEM(shared_up.shape, half),
            pltpu.VMEM(shared_down.shape, half),
            pltpu.VMEM((2 * rows, hid), half),
            pltpu.VMEM((rows, width), half),
            pltpu.VMEM((rows, width), jnp.float32),
            dma((6,)),
            dma((experts, pieces)),
            dma((2, pieces)),
            dma((zs, pieces)),
            dma((zs, pieces)),
            dma((2 * zs, pieces)),
            dma((experts,)),
            dma((experts,)),
            dma((2 * zs,)),
            dma((2 * zs,)),
            dma((zs, pieces)),
            dma((zs, pieces)),
            dma((zs, pieces)),
            dma((zs + 1, pieces)),
        ],
        compiler_params=pltpu.CompilerParams(
            collective_id=0, has_side_effects=True, vmem_limit_bytes=60 * 1024 * 1024
        ),
    )(
        second_normed, middle, weights,
        expert_gate, expert_up, expert_down, shared_gate, shared_up, shared_down,
    )


def mixer_kernel(
    tokens, prior, mix_gain, in_weight, params, input_map, output_map, skip, out_weight,
    channel_gain, new_state, middle, second, normed, acts, acc,
):
    step = pl.program_id(0)
    lane = 128
    channels = in_weight.shape[1]
    width = input_map.shape[2]
    group = acts.shape[1] * width // prior.shape[2]
    per = lane // group
    states = per * width

    def scaled(values, gain):
        factor = lax.rsqrt(jnp.mean(values * values, axis=-1, keepdims=True) + norm_eps)
        return (values * factor * gain[...]).astype(jnp.bfloat16)

    @pl.when(step == 0)
    def _():
        normed[...] = scaled(tokens[...].astype(jnp.float32), mix_gain)
        acc[...] = jnp.zeros_like(acc)

    drive = jnp.dot(normed[...], in_weight[...], preferred_element_type=jnp.float32)
    drive = drive.astype(jnp.bfloat16)
    row = lax.broadcasted_iota(jnp.int32, (lane, states), 0) // group
    column = lax.broadcasted_iota(jnp.int32, (lane, states), 1) // width
    own_group = row == column

    def spread(table):
        tiled = jnp.concatenate([table] * per, axis=1)
        return jnp.where(own_group, tiled, 0.0).astype(jnp.bfloat16)

    for sub in range(channels // lane):
        cols = slice(sub * lane, (sub + 1) * lane)
        ent = slice(sub * states, (sub + 1) * states)
        part = drive[:, cols]
        push_real = jnp.dot(
            part, spread(input_map[0, cols, :]), preferred_element_type=jnp.float32
        )
        push_imag = jnp.dot(
            part, spread(input_map[1, cols, :]), preferred_element_type=jnp.float32
        )
        turn_real, turn_imag = params[0:1, ent], params[1:2, ent]
        hold_real, hold_imag = params[2:3, ent], params[3:4, ent]
        old_real, old_imag = prior[0, :, ent], prior[1, :, ent]
        fresh_real = (
            turn_real * old_real - turn_imag * old_imag
            + (push_real * hold_real - push_imag * hold_imag)
        )
        fresh_imag = (
            turn_real * old_imag + turn_imag * old_real
            + (push_real * hold_imag + push_imag * hold_real)
        )
        new_state[0, :, ent] = fresh_real
        new_state[1, :, ent] = fresh_imag
        across = (((1,), (1,)), ((), ()))
        readout = lax.dot_general(
            fresh_real.astype(jnp.bfloat16), spread(output_map[0, cols, :]), across,
            preferred_element_type=jnp.float32,
        ) - lax.dot_general(
            fresh_imag.astype(jnp.bfloat16), spread(output_map[1, cols, :]), across,
            preferred_element_type=jnp.float32,
        )
        readout = readout + skip[:, cols] * part.astype(jnp.float32)
        acts[:, cols] = jax.nn.gelu(readout).astype(jnp.bfloat16)
    acc[...] += jnp.dot(acts[...], out_weight[...], preferred_element_type=jnp.float32)

    @pl.when(step == pl.num_programs(0) - 1)
    def _():
        mixed = acc[...].astype(jnp.bfloat16).astype(jnp.float32)
        mid = (tokens[...].astype(jnp.float32) + mixed).astype(jnp.bfloat16)
        middle[...] = mid
        second[...] = scaled(mid.astype(jnp.float32), channel_gain)


def mixer_stage(
    tokens, prior_state, mix_gain, in_weight, decay_rate, frequency, log_step,
    input_map, output_map, skip_gain, out_weight, channel_gain,
):
    rows, model = tokens.shape
    groups, width = decay_rate.shape
    channels = in_weight.shape[1]
    step_size = jnp.exp(log_step)[:, None]
    real_rate = -decay_rate
    magnitude = jnp.exp(real_rate * step_size)
    turn_real = magnitude * jnp.cos(frequency * step_size)
    turn_imag = magnitude * jnp.sin(frequency * step_size)
    denominator = real_rate * real_rate + frequency * frequency
    hold_real = ((turn_real - 1.0) * real_rate + turn_imag * frequency) / denominator
    hold_imag = (turn_imag * real_rate - (turn_real - 1.0) * frequency) / denominator
    params = jnp.stack([turn_real, turn_imag, hold_real, hold_imag]).reshape(4, -1)
    in_map = jnp.transpose(input_map, (0, 1, 3, 2)).reshape(2, channels, width)
    out_map = output_map.reshape(2, channels, width)
    block = 256
    states = block * groups * width // channels

    def whole(*shape):
        return pl.BlockSpec(shape, lambda i: (0,) * len(shape))

    half = jnp.bfloat16
    return pl.pallas_call(
        mixer_kernel,
        grid=(channels // block,),
        out_shape=(
            jax.ShapeDtypeStruct(prior_state.shape, jnp.float32),
            jax.ShapeDtypeStruct((rows, model), half),
            jax.ShapeDtypeStruct((rows, model), half),
        ),
        in_specs=[
            whole(rows, model),
            pl.BlockSpec((2, rows, states), lambda i: (0, 0, i)),
            whole(1, model),
            pl.BlockSpec((model, block), lambda i: (0, i)),
            pl.BlockSpec((4, states), lambda i: (0, i)),
            pl.BlockSpec((2, block, width), lambda i: (0, i, 0)),
            pl.BlockSpec((2, block, width), lambda i: (0, i, 0)),
            pl.BlockSpec((1, block), lambda i: (0, i)),
            pl.BlockSpec((block, model), lambda i: (i, 0)),
            whole(1, model),
        ],
        out_specs=(
            pl.BlockSpec((2, rows, states), lambda i: (0, 0, i)),
            whole(rows, model),
            whole(rows, model),
        ),
        scratch_shapes=[
            pltpu.VMEM((rows, model), half),
            pltpu.VMEM((rows, block), half),
            pltpu.VMEM((rows, model), jnp.float32),
        ],
        compiler_params=pltpu.CompilerParams(
            dimension_semantics=("arbitrary",), vmem_limit_bytes=62 * 1024 * 1024
        ),
    )(
        tokens, prior_state, mix_gain[None], in_weight, params, in_map, out_map,
        skip_gain[None], out_weight, channel_gain[None],
    )


def body(
    tokens,
    prior_state,
    mix_gain,
    in_weight,
    decay_rate,
    frequency,
    log_step,
    input_map,
    output_map,
    skip_gain,
    out_weight,
    channel_gain,
    expert_gate,
    expert_up,
    expert_down,
    shared_gate,
    shared_up,
    shared_down,
    routes,
    route_weights,
):
    if lax.axis_size("tp") == 1 and lax.axis_size("ep") == 16:
        new_state, middle, second_normed = mixer_stage(
            tokens, prior_state, mix_gain, in_weight, decay_rate, frequency, log_step,
            input_map, output_map, skip_gain, out_weight, channel_gain,
        )
        layer_out = expert_stage(
            second_normed, middle, routes, route_weights,
            expert_gate, expert_up, expert_down, shared_gate, shared_up, shared_down,
        )
        return (layer_out, new_state)
    normed = root_scale(tokens, mix_gain)
    drive_rows = jnp.dot(normed, in_weight, preferred_element_type=jnp.float32).astype(jnp.bfloat16)
    readout, new_state = state_update(
        drive_rows, prior_state, decay_rate, frequency, log_step, input_map, output_map, skip_gain
    )
    activated = jax.nn.gelu(readout).astype(jnp.bfloat16)
    partial_value = jnp.dot(activated, out_weight, preferred_element_type=jnp.float32)
    mixer_out = lax.psum(partial_value.astype(jnp.bfloat16), "tp").astype(jnp.float32)
    middle = (tokens.astype(jnp.float32) + mixer_out).astype(jnp.bfloat16)
    second_normed = root_scale(middle, channel_gain)
    shared_gval = jnp.dot(second_normed, shared_gate, preferred_element_type=jnp.float32)
    shared_uval = jnp.dot(second_normed, shared_up, preferred_element_type=jnp.float32)
    shared_hidden = (jax.nn.silu(shared_gval) * shared_uval).astype(jnp.bfloat16)
    shared_piece = jnp.dot(shared_hidden, shared_down, preferred_element_type=jnp.float32)
    shared_out = lax.psum_scatter(
        shared_piece.astype(jnp.bfloat16), "tp", scatter_dimension=1, tiled=True
    ).astype(jnp.float32)
    half_cols = second_normed.shape[1] // lax.axis_size("tp")
    routed = exchanged_experts(
        second_normed, routes, route_weights, expert_gate, expert_up, expert_down
    )
    own_middle = lax.dynamic_slice_in_dim(middle, lax.axis_index("tp") * half_cols, half_cols, 1)
    layer_out = (own_middle.astype(jnp.float32) + routed + shared_out).astype(jnp.bfloat16)
    return (layer_out, new_state)


def solution(mesh):
    in_specs = (
        P(("grp", "ep"), None),
        P(None, ("grp", "ep"), "tp"),
        P(),
        P(None, "tp"),
        P("tp", None),
        P("tp", None),
        P("tp"),
        P(None, "tp", None, None),
        P(None, "tp", None, None),
        P("tp"),
        P("tp", None),
        P(),
        P("ep", None, "tp"),
        P("ep", None, "tp"),
        P("ep", "tp", None),
        P(None, "tp"),
        P(None, "tp"),
        P("tp", None),
        P(("grp", "ep"), None),
        P(("grp", "ep"), None),
    )
    out_specs = (P(("grp", "ep"), "tp"), P(None, ("grp", "ep"), "tp"))
    return jax.shard_map(body, mesh=mesh, in_specs=in_specs, out_specs=out_specs, check_vma=False)
```

```python
import functools
import jax
import jax.numpy as jnp
from jax import lax
from jax.experimental import pallas as pl
from jax.experimental.pallas import tpu as pltpu
from jax.sharding import PartitionSpec as P

norm_eps = 1e-06
highest = lax.Precision.HIGHEST
MESH = pl.DeviceIdType.MESH


def root_scale(activations, scale_gain):
    values = activations.astype(jnp.float32)
    factor = lax.rsqrt(jnp.mean(values * values, axis=-1, keepdims=True) + norm_eps)
    return (values * factor * scale_gain).astype(jnp.bfloat16)


def state_update(
    drive_rows, prior_state, decay_rate, frequency, log_step, input_map, output_map, skip_gain
):
    sequences = drive_rows.shape[0]
    groups = decay_rate.shape[0]
    driven = drive_rows.astype(jnp.float32).reshape(sequences, groups, -1)
    step_size = jnp.exp(log_step)[:, None]
    real_rate = -decay_rate
    magnitude = jnp.exp(real_rate * step_size)
    turn_real = magnitude * jnp.cos(frequency * step_size)
    turn_imag = magnitude * jnp.sin(frequency * step_size)
    denominator = real_rate * real_rate + frequency * frequency
    hold_real = ((turn_real - 1.0) * real_rate + turn_imag * frequency) / denominator
    hold_imag = (turn_imag * real_rate - (turn_real - 1.0) * frequency) / denominator
    push_real = jnp.einsum("sgh,gph->sgp", driven, input_map[0], precision=highest)
    push_imag = jnp.einsum("sgh,gph->sgp", driven, input_map[1], precision=highest)
    enter_real = push_real * hold_real - push_imag * hold_imag
    enter_imag = push_real * hold_imag + push_imag * hold_real
    old_real = prior_state[0].reshape(sequences, groups, -1)
    old_imag = prior_state[1].reshape(sequences, groups, -1)
    fresh_real = turn_real * old_real - turn_imag * old_imag + enter_real
    fresh_imag = turn_real * old_imag + turn_imag * old_real + enter_imag
    readout = jnp.einsum("ghp,sgp->sgh", output_map[0], fresh_real, precision=highest)
    readout = readout - jnp.einsum("ghp,sgp->sgh", output_map[1], fresh_imag, precision=highest)
    readout = readout.reshape(sequences, -1) + skip_gain * drive_rows.astype(jnp.float32)
    fresh = jnp.stack([fresh_real.reshape(sequences, -1), fresh_imag.reshape(sequences, -1)])
    return (readout, fresh)


def exchanged_experts(second_normed, routes, route_weights, expert_gate, expert_up, expert_down):
    experts = lax.axis_size("ep")
    seq_rows, top_count = routes.shape
    slot_cap = min(seq_rows, max(2, 3 * seq_rows * top_count // (2 * experts)))
    flat_routes = routes.reshape(-1)
    one_hot = (flat_routes[:, None] == jnp.arange(experts, dtype=jnp.int32)[None, :]).astype(
        jnp.int32
    )
    ranked = jnp.sum((jnp.cumsum(one_hot, axis=0) - one_hot) * one_hot, axis=1)
    slot_index = flat_routes * slot_cap + ranked
    placed = slot_index[:, None] == jnp.arange(experts * slot_cap, dtype=jnp.int32)[None, :]
    placed_rows = jnp.any(placed.reshape(seq_rows, top_count, experts * slot_cap), axis=1).astype(
        jnp.bfloat16
    )
    outgoing = lax.dot_general(
        placed_rows, second_normed, (((0,), (0,)), ((), ())), preferred_element_type=jnp.float32
    ).astype(jnp.bfloat16)
    outgoing = outgoing.reshape(experts, slot_cap, -1)
    arrived = lax.all_to_all(outgoing, "ep", split_axis=0, concat_axis=0, tiled=True)
    sources, count_items, full_width = arrived.shape
    expert_rows = arrived.reshape(sources * count_items, full_width)
    gate_val = jnp.dot(expert_rows, expert_gate[0], preferred_element_type=jnp.float32)
    up_val = jnp.dot(expert_rows, expert_up[0], preferred_element_type=jnp.float32)
    hidden = (jax.nn.silu(gate_val) * up_val).astype(jnp.bfloat16)
    piece = jnp.dot(hidden, expert_down[0], preferred_element_type=jnp.float32)
    summed = lax.psum_scatter(
        piece.reshape(sources, count_items, full_width).astype(jnp.bfloat16),
        "tp",
        scatter_dimension=2,
        tiled=True,
    )
    returned = lax.all_to_all(summed, "ep", split_axis=0, concat_axis=0, tiled=True)
    flat_back = returned.reshape(experts * slot_cap, -1)
    picked = (
        jnp.take(flat_back, slot_index, axis=0).reshape(seq_rows, top_count, -1).astype(jnp.float32)
    )
    routed = jnp.einsum("sk,skd->sd", route_weights, picked)
    return routed


def near_first(extent):
    return [sorted(range(extent), key=lambda other: (abs(other - at), min(other, extent - 1 - other))) for at in range(extent)]


def looked_up(table, position):
    found = jnp.int32(0)
    for at, entry in enumerate(table):
        found = jnp.where(position == at, jnp.int32(entry), found)
    return found


def expert_kernel(
    grid_shape, pieces,
    own, middle, weights, gate_in, up_in, down_in, sgate_in, sup_in, sdown_in,
    out,
    rows_all, back, from_twin, from_side, from_far, weight_all,
    gate, up, down, sgate, sup, sdown, hidden, shared, total,
    load_sem, row_recv, own_z_send, fwd_z_send, fwd_x_send, fwd_twin_send,
    w_send, w_recv, twin_send, twin_recv, side_send, side_recv, far_send, far_recv,
):
    zs, xs, cs = grid_shape
    count = zs * xs * cs
    me = lax.axis_index("ep")
    core = lax.rem(me, cs)
    col = lax.rem(me // cs, xs)
    level = me // (cs * xs)
    rows, width = own.shape
    span = rows // pieces
    hid = gate.shape[1]

    def device(z, x, c):
        return (z * xs + x) * cs + c

    twin = device(level, col, 1 - core)
    side = device(level, 1 - col, core)
    order = [looked_up([row[j] for row in near_first(zs)], level) for j in range(zs)]

    def part(base, h):
        return pl.ds(pl.multiple_of(base * rows + h * span, 16), span)

    loads = [
        pltpu.make_async_copy(src, dst, load_sem.at[n])
        for n, (src, dst) in enumerate(
            ((gate_in.at[0], gate), (up_in.at[0], up), (down_in.at[0], down),
             (sgate_in, sgate), (sup_in, sup), (sdown_in, sdown))
        )
    ]
    for load in loads:
        load.start()

    barrier = pltpu.get_barrier_semaphore()
    for step in range(1, count):
        pl.semaphore_signal(
            barrier, inc=1, device_id={"ep": lax.rem(me + step, count)}, device_id_type=MESH
        )
    pl.semaphore_wait(barrier, count - 1)

    def remote(src, dst, send, recv, target):
        return pltpu.make_async_remote_copy(
            src_ref=src, dst_ref=dst, send_sem=send, recv_sem=recv,
            device_id={"ep": target}, device_id_type=MESH,
        )

    sent = []

    def push(src, dst, send, recv, target):
        copy = remote(src, dst, send, recv, target)
        copy.start()
        sent.append(copy)

    def row_copy(src_ref, src_rows, origin, h, send, target):
        return remote(
            src_ref.at[src_rows], rows_all.at[part(origin, h)], send, row_recv.at[origin, h], target
        )

    for h in range(pieces):
        piece = pl.ds(h * span, span)

        @pl.when(level > 0)
        def _():
            row_copy(own, piece, me, h, own_z_send.at[0, h], device(level - 1, col, core)).start()

        @pl.when(level < zs - 1)
        def _():
            row_copy(own, piece, me, h, own_z_send.at[1, h], device(level + 1, col, core)).start()

        for send, target in ((fwd_x_send.at[0, h], side), (fwd_twin_send.at[0, h], twin)):
            copy = row_copy(own, piece, me, h, send, target)
            copy.start()
            sent.append(copy)

    for step in range(1, count):
        other = lax.rem(me + step, count)
        push(
            weights.at[other], weight_all.at[me], w_send.at[step], w_recv.at[count - step], other
        )
    rows_all[part(me, 0), :] = own[pl.ds(0, span), :]
    for h in range(1, pieces):
        rows_all[part(me, h), :] = own[pl.ds(h * span, span), :]
    weight_all[me] = weights[me]

    def arrived(origin, h):
        row_copy(own, pl.ds(h * span, span), origin, h, own_z_send.at[0, h], twin).wait_recv()

    def feed(source, take, gate_w, up_w, down_w, finish):
        def first(n, carry):
            cols = pl.ds(pl.multiple_of(n * 256, 256), 256)
            data = source()
            g = jnp.dot(data, gate_w[:, cols], preferred_element_type=jnp.float32)
            u = jnp.dot(data, up_w[:, cols], preferred_element_type=jnp.float32)
            hidden[pl.ds(0, take), cols] = (jax.nn.silu(g) * u).astype(jnp.bfloat16)
            return carry

        lax.fori_loop(0, hid // 256, first, 0)

        def second(n, carry):
            cols = pl.ds(pl.multiple_of(n * 512, 512), 512)
            piece = jnp.dot(
                hidden[pl.ds(0, take), :], down_w[:, cols], preferred_element_type=jnp.float32
            )
            finish(cols, piece.astype(jnp.bfloat16))
            return carry

        lax.fori_loop(0, width // 512, second, 0)

    def chip(label, z, x):
        base = device(z, x, 0)
        block = pl.ds(pl.multiple_of(base * rows, 16), cs * rows)
        scales = []
        for c in range(cs):
            line = jnp.broadcast_to(weight_all[base + c], (128, 128))
            scales.append(jnp.transpose(line)[:rows])
        scale = jnp.concatenate(scales, axis=0)
        scale = jnp.concatenate([scale] * 4, axis=1)

        def finish(cols, piece):
            back[block, cols] = (piece.astype(jnp.float32) * scale).astype(jnp.bfloat16)

        feed(lambda: rows_all[block, :], cs * rows, gate, up, down, finish)
        push(
            back.at[part_all(device(z, x, 1 - core))],
            from_twin.at[label],
            twin_send.at[label],
            twin_recv.at[label],
            twin,
        )

    def part_all(origin):
        return pl.ds(pl.multiple_of(origin * rows, 16), rows)

    def keep(cols, piece):
        shared[:, cols] = piece

    def pair_in(z, x):
        for h in range(pieces):
            arrived(device(z, x, 1 - core), h)

    def onward_of(j):
        return jnp.where(order[j] < level, level + 1, level - 1)

    def fwd_copies(j, h):
        origin = device(order[j], col, core)
        return [
            row_copy(rows_all, part(origin, h), origin, h, send, target)
            for send, target in ((fwd_x_send.at[j, h], side), (fwd_twin_send.at[j, h], twin))
        ]

    def fwd(j):
        for h in range(pieces):
            fwd_piece(j, h)

    def fwd_piece(j, h):
        origin = device(order[j], col, core)
        arrived(origin, h)
        onward = onward_of(j)

        @pl.when((onward >= 0) & (onward < zs))
        def _():
            row_copy(
                rows_all, part(origin, h), origin, h, fwd_z_send.at[j, h],
                device(onward, col, core),
            ).start()

        for copy in fwd_copies(j, h):
            copy.start()

    def across_in(j):
        across = device(order[j], 1 - col, core)
        for h in range(pieces):
            arrived(across, h)
            copy = row_copy(rows_all, part(across, h), across, h, fwd_twin_send.at[zs + j, h], twin)
            copy.start()
            sent.append(copy)

    def own_chip(j):
        pair_in(order[j], col)
        chip(j, order[j], col)

    def across_chip(j):
        pair_in(order[j], 1 - col)
        chip(zs + j, order[j], 1 - col)

    inner = (level > 0) & (level < zs - 1)
    outer = (level == 0) | (level == zs - 1)

    for load in loads[:3]:
        load.wait()
    for step in range(1, count):
        remote(
            weights.at[me], weight_all.at[lax.rem(me + step, count)],
            w_send.at[step], w_recv.at[step], twin,
        ).wait_recv()
    own_chip(0)
    for h in range(pieces):
        fwd_piece(1, h)
        pl.when(inner)(functools.partial(fwd_piece, 2, h))
        if h == 0:
            for load in loads[3:]:
                load.wait()
            feed(lambda: own[...], rows, sgate, sup, sdown, keep)
    across_in(0)
    own_chip(1)
    across_chip(0)
    for h in range(pieces):
        pl.when(inner)(functools.partial(fwd_piece, 3, h))
        pl.when(outer)(functools.partial(fwd_piece, 2, h))
    across_in(1)
    own_chip(2)
    across_chip(1)
    pl.when(outer)(functools.partial(fwd, 3))
    across_in(2)
    own_chip(3)
    across_chip(2)

    def twin_in(label):
        remote(
            from_twin.at[label], from_twin.at[label], twin_send.at[label], twin_recv.at[label], twin
        ).wait_recv()

    def added(first, others, store):
        def strip(n, carry):
            at = pl.multiple_of(n * 16, 16)
            value = first(at).astype(jnp.float32)
            for other in others:
                value = value + other(at).astype(jnp.float32)
            store(at, value)
            return carry

        lax.fori_loop(0, span // 16, strip, 0)

    def back_at(origin, h):
        return lambda at: back[pl.ds(pl.multiple_of(origin * rows + h * span + at, 16), 16), :]

    def slot_at(ref, slot, h):
        return lambda at: ref[slot, pl.ds(pl.multiple_of(h * span + at, 16), 16), :]

    def to_back(origin, h):
        def store(at, value):
            back[pl.ds(pl.multiple_of(origin * rows + h * span + at, 16), 16), :] = value.astype(
                jnp.bfloat16
            )

        return store

    def side_out(j):
        twin_in(zs + j)
        origin = device(order[j], 1 - col, core)
        for h in range(pieces):
            added(back_at(origin, h), [slot_at(from_twin, zs + j, h)], to_back(origin, h))
            push(
                back.at[part(origin, h)], from_side.at[j, pl.ds(h * span, span)],
                side_send.at[j, h], side_recv.at[j, h], side,
            )

    side_out(2)
    across_in(3)
    across_chip(3)
    for j in (3, 1, 0):
        side_out(j)

    def side_in(j, h):
        view = from_side.at[j, pl.ds(h * span, span)]
        remote(view, view, side_send.at[j, h], side_recv.at[j, h], side).wait_recv()

    def far_in(slot, h):
        view = from_far.at[slot, pl.ds(h * span, span)]
        remote(view, view, far_send.at[0, h], far_recv.at[slot, h], side).wait_recv()

    for j in (2, 3, 1):
        twin_in(j)
        goal = order[j]
        origin = device(goal, col, core)
        nearer = jnp.where(goal < level, level - 1, level + 1)
        behind = jnp.where(goal < level, level + 1, level - 1)
        slot = jnp.where((nearer == goal) & (goal > level), zs, goal)
        for h in range(pieces):
            side_in(j, h)
            terms = [slot_at(from_twin, j, h), slot_at(from_side, j, h)]

            @pl.when((behind >= 0) & (behind < zs))
            def _():
                far_in(goal, h)
                added(
                    back_at(origin, h), terms + [slot_at(from_far, goal, h)], to_back(origin, h)
                )

            @pl.when((behind < 0) | (behind >= zs))
            def _():
                added(back_at(origin, h), terms, to_back(origin, h))

            push(
                back.at[part(origin, h)], from_far.at[slot, pl.ds(h * span, span)],
                far_send.at[j, h], far_recv.at[slot, h], device(nearer, col, core),
            )
    twin_in(0)
    for h in range(pieces):
        side_in(0, h)

        def to_total(at, value):
            total[pl.ds(pl.multiple_of(h * span + at, 16), 16), :] = value

        def total_at(at):
            return total[pl.ds(pl.multiple_of(h * span + at, 16), 16), :]

        added(back_at(me, h), [slot_at(from_twin, 0, h), slot_at(from_side, 0, h)], to_total)

        @pl.when(level > 0)
        def _():
            far_in(zs, h)
            added(total_at, [slot_at(from_far, zs, h)], to_total)

        @pl.when(level < zs - 1)
        def _():
            far_in(level, h)
            added(total_at, [slot_at(from_far, level, h)], to_total)

        def plain(ref):
            return lambda at: ref[pl.ds(pl.multiple_of(h * span + at, 16), 16), :]

        def to_out(at, value):
            out[pl.ds(pl.multiple_of(h * span + at, 16), 16), :] = value.astype(jnp.bfloat16)

        added(plain(middle), [total_at, plain(shared)], to_out)

    for copy in sent:
        copy.wait_send()
    for h in range(pieces):
        piece = pl.ds(h * span, span)

        @pl.when(level > 0)
        def _():
            row_copy(own, piece, me, h, own_z_send.at[0, h], twin).wait_send()

        @pl.when(level < zs - 1)
        def _():
            row_copy(own, piece, me, h, own_z_send.at[1, h], twin).wait_send()

        for j in range(1, zs):
            for copy in fwd_copies(j, h):
                copy.wait_send()
            onward = onward_of(j)

            @pl.when((onward >= 0) & (onward < zs))
            def _():
                row_copy(own, piece, me, h, fwd_z_send.at[j, h], twin).wait_send()


def expert_stage(
    second_normed, middle, routes, route_weights,
    expert_gate, expert_up, expert_down, shared_gate, shared_up, shared_down,
):
    experts = lax.axis_size("ep")
    grid_shape = (experts // 4, 2, 2)
    zs = grid_shape[0]
    rows, width = second_normed.shape
    hid = expert_gate.shape[2]
    pieces = 2 if rows % 32 == 0 else 1
    chosen = routes[None, :, :] == jnp.arange(experts, dtype=jnp.int32)[:, None, None]
    weights = jnp.sum(jnp.where(chosen, route_weights[None], 0.0), axis=2)
    weights = jnp.pad(weights, ((0, 0), (0, 128 - rows)))[:, None, :]
    vmem = pl.BlockSpec(memory_space=pltpu.VMEM)
    hbm = pl.BlockSpec(memory_space=pl.ANY)
    dma = pltpu.SemaphoreType.DMA
    half = jnp.bfloat16
    return pl.pallas_call(
        functools.partial(expert_kernel, grid_shape, pieces),
        out_shape=jax.ShapeDtypeStruct((rows, width), half),
        in_specs=[vmem] * 3 + [hbm] * 6,
        out_specs=vmem,
        scratch_shapes=[
            pltpu.VMEM((experts * rows, width), half),
            pltpu.VMEM((experts * rows, width), half),
            pltpu.VMEM((2 * zs, rows, width), half),
            pltpu.VMEM((zs, rows, width), half),
            pltpu.VMEM((zs + 1, rows, width), half),
            pltpu.VMEM((experts, 1, 128), jnp.float32),
            pltpu.VMEM((width, hid), half),
            pltpu.VMEM((width, hid), half),
            pltpu.VMEM((hid, width), half),
            pltpu.VMEM(shared_gate.shape, half),
            pltpu.VMEM(shared_up.shape, half),
            pltpu.VMEM(shared_down.shape, half),
            pltpu.VMEM((2 * rows, hid), half),
            pltpu.VMEM((rows, width), half),
            pltpu.VMEM((rows, width), jnp.float32),
            dma((6,)),
            dma((experts, pieces)),
            dma((2, pieces)),
            dma((zs, pieces)),
            dma((zs, pieces)),
            dma((2 * zs, pieces)),
            dma((experts,)),
            dma((experts,)),
            dma((2 * zs,)),
            dma((2 * zs,)),
            dma((zs, pieces)),
            dma((zs, pieces)),
            dma((zs, pieces)),
            dma((zs + 1, pieces)),
        ],
        compiler_params=pltpu.CompilerParams(
            collective_id=0, has_side_effects=True, vmem_limit_bytes=60 * 1024 * 1024
        ),
    )(
        second_normed, middle, weights,
        expert_gate, expert_up, expert_down, shared_gate, shared_up, shared_down,
    )


def mixer_kernel(
    tokens, prior, mix_gain, in_weight, params, input_map, output_map, skip, out_weight,
    channel_gain, new_state, middle, second, normed, acts, acc,
):
    step = pl.program_id(0)
    lane = 128
    channels = in_weight.shape[1]
    width = input_map.shape[2]
    group = acts.shape[1] * width // prior.shape[2]
    per = lane // group
    states = per * width

    def scaled(values, gain):
        factor = lax.rsqrt(jnp.mean(values * values, axis=-1, keepdims=True) + norm_eps)
        return (values * factor * gain[...]).astype(jnp.bfloat16)

    @pl.when(step == 0)
    def _():
        normed[...] = scaled(tokens[...].astype(jnp.float32), mix_gain)
        acc[...] = jnp.zeros_like(acc)

    drive = jnp.dot(normed[...], in_weight[...], preferred_element_type=jnp.float32)
    drive = drive.astype(jnp.bfloat16)
    row = lax.broadcasted_iota(jnp.int32, (lane, states), 0) // group
    column = lax.broadcasted_iota(jnp.int32, (lane, states), 1) // width
    own_group = row == column

    def spread(table):
        tiled = jnp.concatenate([table] * per, axis=1)
        return jnp.where(own_group, tiled, 0.0).astype(jnp.bfloat16)

    for sub in range(channels // lane):
        cols = slice(sub * lane, (sub + 1) * lane)
        ent = slice(sub * states, (sub + 1) * states)
        part = drive[:, cols]
        push_real = jnp.dot(
            part, spread(input_map[0, cols, :]), preferred_element_type=jnp.float32
        )
        push_imag = jnp.dot(
            part, spread(input_map[1, cols, :]), preferred_element_type=jnp.float32
        )
        turn_real, turn_imag = params[0:1, ent], params[1:2, ent]
        hold_real, hold_imag = params[2:3, ent], params[3:4, ent]
        old_real, old_imag = prior[0, :, ent], prior[1, :, ent]
        fresh_real = (
            turn_real * old_real - turn_imag * old_imag
            + (push_real * hold_real - push_imag * hold_imag)
        )
        fresh_imag = (
            turn_real * old_imag + turn_imag * old_real
            + (push_real * hold_imag + push_imag * hold_real)
        )
        new_state[0, :, ent] = fresh_real
        new_state[1, :, ent] = fresh_imag
        across = (((1,), (1,)), ((), ()))
        readout = lax.dot_general(
            fresh_real.astype(jnp.bfloat16), spread(output_map[0, cols, :]), across,
            preferred_element_type=jnp.float32,
        ) - lax.dot_general(
            fresh_imag.astype(jnp.bfloat16), spread(output_map[1, cols, :]), across,
            preferred_element_type=jnp.float32,
        )
        readout = readout + skip[:, cols] * part.astype(jnp.float32)
        acts[:, cols] = jax.nn.gelu(readout).astype(jnp.bfloat16)
    acc[...] += jnp.dot(acts[...], out_weight[...], preferred_element_type=jnp.float32)

    @pl.when(step == pl.num_programs(0) - 1)
    def _():
        mixed = acc[...].astype(jnp.bfloat16).astype(jnp.float32)
        mid = (tokens[...].astype(jnp.float32) + mixed).astype(jnp.bfloat16)
        middle[...] = mid
        second[...] = scaled(mid.astype(jnp.float32), channel_gain)


def mixer_stage(
    tokens, prior_state, mix_gain, in_weight, decay_rate, frequency, log_step,
    input_map, output_map, skip_gain, out_weight, channel_gain,
):
    rows, model = tokens.shape
    groups, width = decay_rate.shape
    channels = in_weight.shape[1]
    step_size = jnp.exp(log_step)[:, None]
    real_rate = -decay_rate
    magnitude = jnp.exp(real_rate * step_size)
    turn_real = magnitude * jnp.cos(frequency * step_size)
    turn_imag = magnitude * jnp.sin(frequency * step_size)
    denominator = real_rate * real_rate + frequency * frequency
    hold_real = ((turn_real - 1.0) * real_rate + turn_imag * frequency) / denominator
    hold_imag = (turn_imag * real_rate - (turn_real - 1.0) * frequency) / denominator
    params = jnp.stack([turn_real, turn_imag, hold_real, hold_imag]).reshape(4, -1)
    in_map = jnp.transpose(input_map, (0, 1, 3, 2)).reshape(2, channels, width)
    out_map = output_map.reshape(2, channels, width)
    block = 256
    states = block * groups * width // channels

    def whole(*shape):
        return pl.BlockSpec(shape, lambda i: (0,) * len(shape))

    half = jnp.bfloat16
    return pl.pallas_call(
        mixer_kernel,
        grid=(channels // block,),
        out_shape=(
            jax.ShapeDtypeStruct(prior_state.shape, jnp.float32),
            jax.ShapeDtypeStruct((rows, model), half),
            jax.ShapeDtypeStruct((rows, model), half),
        ),
        in_specs=[
            whole(rows, model),
            pl.BlockSpec((2, rows, states), lambda i: (0, 0, i)),
            whole(1, model),
            pl.BlockSpec((model, block), lambda i: (0, i)),
            pl.BlockSpec((4, states), lambda i: (0, i)),
            pl.BlockSpec((2, block, width), lambda i: (0, i, 0)),
            pl.BlockSpec((2, block, width), lambda i: (0, i, 0)),
            pl.BlockSpec((1, block), lambda i: (0, i)),
            pl.BlockSpec((block, model), lambda i: (i, 0)),
            whole(1, model),
        ],
        out_specs=(
            pl.BlockSpec((2, rows, states), lambda i: (0, 0, i)),
            whole(rows, model),
            whole(rows, model),
        ),
        scratch_shapes=[
            pltpu.VMEM((rows, model), half),
            pltpu.VMEM((rows, block), half),
            pltpu.VMEM((rows, model), jnp.float32),
        ],
        compiler_params=pltpu.CompilerParams(
            dimension_semantics=("arbitrary",), vmem_limit_bytes=62 * 1024 * 1024
        ),
    )(
        tokens, prior_state, mix_gain[None], in_weight, params, in_map, out_map,
        skip_gain[None], out_weight, channel_gain[None],
    )


def body(
    tokens,
    prior_state,
    mix_gain,
    in_weight,
    decay_rate,
    frequency,
    log_step,
    input_map,
    output_map,
    skip_gain,
    out_weight,
    channel_gain,
    expert_gate,
    expert_up,
    expert_down,
    shared_gate,
    shared_up,
    shared_down,
    routes,
    route_weights,
):
    if lax.axis_size("tp") == 1 and lax.axis_size("ep") == 16:
        new_state, middle, second_normed = mixer_stage(
            tokens, prior_state, mix_gain, in_weight, decay_rate, frequency, log_step,
            input_map, output_map, skip_gain, out_weight, channel_gain,
        )
        layer_out = expert_stage(
            second_normed, middle, routes, route_weights,
            expert_gate, expert_up, expert_down, shared_gate, shared_up, shared_down,
        )
        return (layer_out, new_state)
    normed = root_scale(tokens, mix_gain)
    drive_rows = jnp.dot(normed, in_weight, preferred_element_type=jnp.float32).astype(jnp.bfloat16)
    readout, new_state = state_update(
        drive_rows, prior_state, decay_rate, frequency, log_step, input_map, output_map, skip_gain
    )
    activated = jax.nn.gelu(readout).astype(jnp.bfloat16)
    partial_value = jnp.dot(activated, out_weight, preferred_element_type=jnp.float32)
    mixer_out = lax.psum(partial_value.astype(jnp.bfloat16), "tp").astype(jnp.float32)
    middle = (tokens.astype(jnp.float32) + mixer_out).astype(jnp.bfloat16)
    second_normed = root_scale(middle, channel_gain)
    shared_gval = jnp.dot(second_normed, shared_gate, preferred_element_type=jnp.float32)
    shared_uval = jnp.dot(second_normed, shared_up, preferred_element_type=jnp.float32)
    shared_hidden = (jax.nn.silu(shared_gval) * shared_uval).astype(jnp.bfloat16)
    shared_piece = jnp.dot(shared_hidden, shared_down, preferred_element_type=jnp.float32)
    shared_out = lax.psum_scatter(
        shared_piece.astype(jnp.bfloat16), "tp", scatter_dimension=1, tiled=True
    ).astype(jnp.float32)
    half_cols = second_normed.shape[1] // lax.axis_size("tp")
    routed = exchanged_experts(
        second_normed, routes, route_weights, expert_gate, expert_up, expert_down
    )
    own_middle = lax.dynamic_slice_in_dim(middle, lax.axis_index("tp") * half_cols, half_cols, 1)
    layer_out = (own_middle.astype(jnp.float32) + routed + shared_out).astype(jnp.bfloat16)
    return (layer_out, new_state)


def solution(mesh):
    in_specs = (
        P(("grp", "ep"), None),
        P(None, ("grp", "ep"), "tp"),
        P(),
        P(None, "tp"),
        P("tp", None),
        P("tp", None),
        P("tp"),
        P(None, "tp", None, None),
        P(None, "tp", None, None),
        P("tp"),
        P("tp", None),
        P(),
        P("ep", None, "tp"),
        P("ep", None, "tp"),
        P("ep", "tp", None),
        P(None, "tp"),
        P(None, "tp"),
        P("tp", None),
        P(("grp", "ep"), None),
        P(("grp", "ep"), None),
    )
    out_specs = (P(("grp", "ep"), "tp"), P(None, ("grp", "ep"), "tp"))
    return jax.shard_map(body, mesh=mesh, in_specs=in_specs, out_specs=out_specs, check_vma=False)
```

```python
import functools
import jax
import jax.numpy as jnp
from jax import lax
from jax.experimental import pallas as pl
from jax.experimental.pallas import tpu as pltpu
from jax.sharding import PartitionSpec as P

norm_eps = 1e-06
highest = lax.Precision.HIGHEST
MESH = pl.DeviceIdType.MESH


def root_scale(activations, scale_gain):
    values = activations.astype(jnp.float32)
    factor = lax.rsqrt(jnp.mean(values * values, axis=-1, keepdims=True) + norm_eps)
    return (values * factor * scale_gain).astype(jnp.bfloat16)


def state_update(
    drive_rows, prior_state, decay_rate, frequency, log_step, input_map, output_map, skip_gain
):
    sequences = drive_rows.shape[0]
    groups = decay_rate.shape[0]
    driven = drive_rows.astype(jnp.float32).reshape(sequences, groups, -1)
    step_size = jnp.exp(log_step)[:, None]
    real_rate = -decay_rate
    magnitude = jnp.exp(real_rate * step_size)
    turn_real = magnitude * jnp.cos(frequency * step_size)
    turn_imag = magnitude * jnp.sin(frequency * step_size)
    denominator = real_rate * real_rate + frequency * frequency
    hold_real = ((turn_real - 1.0) * real_rate + turn_imag * frequency) / denominator
    hold_imag = (turn_imag * real_rate - (turn_real - 1.0) * frequency) / denominator
    push_real = jnp.einsum("sgh,gph->sgp", driven, input_map[0], precision=highest)
    push_imag = jnp.einsum("sgh,gph->sgp", driven, input_map[1], precision=highest)
    enter_real = push_real * hold_real - push_imag * hold_imag
    enter_imag = push_real * hold_imag + push_imag * hold_real
    old_real = prior_state[0].reshape(sequences, groups, -1)
    old_imag = prior_state[1].reshape(sequences, groups, -1)
    fresh_real = turn_real * old_real - turn_imag * old_imag + enter_real
    fresh_imag = turn_real * old_imag + turn_imag * old_real + enter_imag
    readout = jnp.einsum("ghp,sgp->sgh", output_map[0], fresh_real, precision=highest)
    readout = readout - jnp.einsum("ghp,sgp->sgh", output_map[1], fresh_imag, precision=highest)
    readout = readout.reshape(sequences, -1) + skip_gain * drive_rows.astype(jnp.float32)
    fresh = jnp.stack([fresh_real.reshape(sequences, -1), fresh_imag.reshape(sequences, -1)])
    return (readout, fresh)


def exchanged_experts(second_normed, routes, route_weights, expert_gate, expert_up, expert_down):
    experts = lax.axis_size("ep")
    seq_rows, top_count = routes.shape
    slot_cap = min(seq_rows, max(2, 3 * seq_rows * top_count // (2 * experts)))
    flat_routes = routes.reshape(-1)
    one_hot = (flat_routes[:, None] == jnp.arange(experts, dtype=jnp.int32)[None, :]).astype(
        jnp.int32
    )
    ranked = jnp.sum((jnp.cumsum(one_hot, axis=0) - one_hot) * one_hot, axis=1)
    slot_index = flat_routes * slot_cap + ranked
    placed = slot_index[:, None] == jnp.arange(experts * slot_cap, dtype=jnp.int32)[None, :]
    placed_rows = jnp.any(placed.reshape(seq_rows, top_count, experts * slot_cap), axis=1).astype(
        jnp.bfloat16
    )
    outgoing = lax.dot_general(
        placed_rows, second_normed, (((0,), (0,)), ((), ())), preferred_element_type=jnp.float32
    ).astype(jnp.bfloat16)
    outgoing = outgoing.reshape(experts, slot_cap, -1)
    arrived = lax.all_to_all(outgoing, "ep", split_axis=0, concat_axis=0, tiled=True)
    sources, count_items, full_width = arrived.shape
    expert_rows = arrived.reshape(sources * count_items, full_width)
    gate_val = jnp.dot(expert_rows, expert_gate[0], preferred_element_type=jnp.float32)
    up_val = jnp.dot(expert_rows, expert_up[0], preferred_element_type=jnp.float32)
    hidden = (jax.nn.silu(gate_val) * up_val).astype(jnp.bfloat16)
    piece = jnp.dot(hidden, expert_down[0], preferred_element_type=jnp.float32)
    summed = lax.psum_scatter(
        piece.reshape(sources, count_items, full_width).astype(jnp.bfloat16),
        "tp",
        scatter_dimension=2,
        tiled=True,
    )
    returned = lax.all_to_all(summed, "ep", split_axis=0, concat_axis=0, tiled=True)
    flat_back = returned.reshape(experts * slot_cap, -1)
    picked = (
        jnp.take(flat_back, slot_index, axis=0).reshape(seq_rows, top_count, -1).astype(jnp.float32)
    )
    routed = jnp.einsum("sk,skd->sd", route_weights, picked)
    return routed


def near_first(extent):
    return [sorted(range(extent), key=lambda other: (abs(other - at), min(other, extent - 1 - other))) for at in range(extent)]


def looked_up(table, position):
    found = jnp.int32(0)
    for at, entry in enumerate(table):
        found = jnp.where(position == at, jnp.int32(entry), found)
    return found


def expert_kernel(
    grid_shape, cuts,
    own, middle, weights, gate_in, up_in, down_in, sgate_in, sup_in, sdown_in,
    out,
    rows_all, back, from_twin, from_side, from_far, from_bent, weight_all,
    gate, up, down, sgate, sup, sdown, hidden, shared, total,
    load_sem, row_recv, own_z_send, fwd_z_send, fwd_x_send, fwd_twin_send,
    w_send, w_recv, twin_send, twin_recv, side_send, side_recv, far_send, far_recv,
    bent_send, bent_far_send, bent_far_recv,
):
    zs, xs, cs = grid_shape
    count = zs * xs * cs
    me = lax.axis_index("ep")
    core = lax.rem(me, cs)
    col = lax.rem(me // cs, xs)
    level = me // (cs * xs)
    rows, width = own.shape
    pieces = len(cuts)
    straight = range(pieces - 1)
    bent = pieces - 1
    hid = gate.shape[1]

    def device(z, x, c):
        return (z * xs + x) * cs + c

    twin = device(level, col, 1 - core)
    side = device(level, 1 - col, core)
    order = [looked_up([row[j] for row in near_first(zs)], level) for j in range(zs)]

    def part(base, h):
        return pl.ds(pl.multiple_of(base * rows + cuts[h][0], 16), cuts[h][1])

    def local(h):
        return pl.ds(cuts[h][0], cuts[h][1])

    loads = [
        pltpu.make_async_copy(src, dst, load_sem.at[n])
        for n, (src, dst) in enumerate(
            ((gate_in.at[0], gate), (up_in.at[0], up), (down_in.at[0], down),
             (sgate_in, sgate), (sup_in, sup), (sdown_in, sdown))
        )
    ]
    for load in loads:
        load.start()

    barrier = pltpu.get_barrier_semaphore()
    for step in range(1, count):
        pl.semaphore_signal(
            barrier, inc=1, device_id={"ep": lax.rem(me + step, count)}, device_id_type=MESH
        )
    pl.semaphore_wait(barrier, count - 1)

    def remote(src, dst, send, recv, target):
        return pltpu.make_async_remote_copy(
            src_ref=src, dst_ref=dst, send_sem=send, recv_sem=recv,
            device_id={"ep": target}, device_id_type=MESH,
        )

    sent = []

    def push(src, dst, send, recv, target):
        copy = remote(src, dst, send, recv, target)
        copy.start()
        sent.append(copy)

    def row_copy(src_ref, src_rows, origin, h, send, target):
        return remote(
            src_ref.at[src_rows], rows_all.at[part(origin, h)], send, row_recv.at[origin, h], target
        )

    for h in (bent, *straight):
        piece = local(h)

        @pl.when(level > 0)
        def _():
            row_copy(own, piece, me, h, own_z_send.at[0, h], device(level - 1, col, core)).start()

        @pl.when(level < zs - 1)
        def _():
            row_copy(own, piece, me, h, own_z_send.at[1, h], device(level + 1, col, core)).start()

        for send, target in ((fwd_x_send.at[0, h], side), (fwd_twin_send.at[0, h], twin)):
            copy = row_copy(own, piece, me, h, send, target)
            copy.start()
            sent.append(copy)

    for step in range(1, count):
        other = lax.rem(me + step, count)
        push(
            weights.at[other], weight_all.at[me], w_send.at[step], w_recv.at[count - step], other
        )
    for h in range(pieces):
        rows_all[part(me, h), :] = own[local(h), :]
    weight_all[me] = weights[me]

    def arrived(origin, h):
        row_copy(own, local(h), origin, h, own_z_send.at[0, h], twin).wait_recv()

    def feed(source, take, gate_w, up_w, down_w, finish):
        def first(n, carry):
            cols = pl.ds(pl.multiple_of(n * 256, 256), 256)
            data = source()
            g = jnp.dot(data, gate_w[:, cols], preferred_element_type=jnp.float32)
            u = jnp.dot(data, up_w[:, cols], preferred_element_type=jnp.float32)
            hidden[pl.ds(0, take), cols] = (jax.nn.silu(g) * u).astype(jnp.bfloat16)
            return carry

        lax.fori_loop(0, hid // 256, first, 0)

        def second(n, carry):
            cols = pl.ds(pl.multiple_of(n * 512, 512), 512)
            piece = jnp.dot(
                hidden[pl.ds(0, take), :], down_w[:, cols], preferred_element_type=jnp.float32
            )
            finish(cols, piece.astype(jnp.bfloat16))
            return carry

        lax.fori_loop(0, width // 512, second, 0)

    def chip(label, z, x):
        base = device(z, x, 0)
        block = pl.ds(pl.multiple_of(base * rows, 16), cs * rows)
        scales = []
        for c in range(cs):
            line = jnp.broadcast_to(weight_all[base + c], (128, 128))
            scales.append(jnp.transpose(line)[:rows])
        scale = jnp.concatenate(scales, axis=0)
        scale = jnp.concatenate([scale] * 4, axis=1)

        def finish(cols, piece):
            back[block, cols] = (piece.astype(jnp.float32) * scale).astype(jnp.bfloat16)

        feed(lambda: rows_all[block, :], cs * rows, gate, up, down, finish)
        push(
            back.at[part_all(device(z, x, 1 - core))],
            from_twin.at[label],
            twin_send.at[label],
            twin_recv.at[label],
            twin,
        )

    def part_all(origin):
        return pl.ds(pl.multiple_of(origin * rows, 16), rows)

    def keep(cols, piece):
        shared[:, cols] = piece

    def pair_in(z, x):
        for h in range(pieces):
            arrived(device(z, x, 1 - core), h)

    def onward_of(j):
        return jnp.where(order[j] < level, level + 1, level - 1)

    def fwd_copies(j, h):
        origin = device(order[j], col, core)
        return [
            row_copy(rows_all, part(origin, h), origin, h, send, target)
            for send, target in ((fwd_twin_send.at[j, h], twin), (fwd_x_send.at[j, h], side))
        ][: 1 if h == bent else 2]

    def fwd(j):
        for h in (bent, *straight):
            fwd_piece(j, h)
        bent_across(j)

    def bent_copies(j):
        origin = device(order[j], 1 - col, core)

        def one(send, target):
            return row_copy(rows_all, part(origin, bent), origin, bent, send, target)

        if j == 0:
            moves = [
                (level > 0, one(bent_send.at[0], device(level - 1, col, core))),
                (level < zs - 1, one(bent_send.at[zs], device(level + 1, col, core))),
            ]
        else:
            onward = onward_of(j)
            moves = [
                ((onward >= 0) & (onward < zs), one(bent_send.at[j], device(onward, col, core)))
            ]
        return moves, one(fwd_twin_send.at[zs + j, bent], twin)

    def bent_across(j):
        arrived(device(order[j], 1 - col, core), bent)
        moves, to_twin = bent_copies(j)
        for allowed, copy in moves:
            pl.when(allowed)(copy.start)
        to_twin.start()

    def fwd_piece(j, h):
        origin = device(order[j], col, core)
        arrived(origin, h)
        onward = onward_of(j)

        @pl.when((onward >= 0) & (onward < zs))
        def _():
            row_copy(
                rows_all, part(origin, h), origin, h, fwd_z_send.at[j, h],
                device(onward, col, core),
            ).start()

        for copy in fwd_copies(j, h):
            copy.start()

    def across_in(j):
        across = device(order[j], 1 - col, core)
        for h in straight:
            arrived(across, h)
            copy = row_copy(rows_all, part(across, h), across, h, fwd_twin_send.at[zs + j, h], twin)
            copy.start()
            sent.append(copy)

    def own_chip(j):
        pair_in(order[j], col)
        chip(j, order[j], col)

    def across_chip(j):
        pair_in(order[j], 1 - col)
        chip(zs + j, order[j], 1 - col)

    inner = (level > 0) & (level < zs - 1)
    outer = (level == 0) | (level == zs - 1)

    for load in loads[:3]:
        load.wait()
    for step in range(1, count):
        remote(
            weights.at[me], weight_all.at[lax.rem(me + step, count)],
            w_send.at[step], w_recv.at[step], twin,
        ).wait_recv()
    own_chip(0)
    bent_across(0)
    for h in (bent, *straight):
        fwd_piece(1, h)
        pl.when(inner)(functools.partial(fwd_piece, 2, h))
        if h == 0:
            for load in loads[3:]:
                load.wait()
            feed(lambda: own[...], rows, sgate, sup, sdown, keep)
    bent_across(1)
    pl.when(inner)(functools.partial(bent_across, 2))
    across_in(0)
    own_chip(1)
    across_chip(0)
    pl.when(inner)(functools.partial(fwd, 3))
    pl.when(outer)(functools.partial(fwd, 2))
    across_in(1)
    own_chip(2)
    across_chip(1)
    pl.when(outer)(functools.partial(fwd, 3))
    across_in(2)
    own_chip(3)
    across_chip(2)

    def twin_in(label):
        remote(
            from_twin.at[label], from_twin.at[label], twin_send.at[label], twin_recv.at[label], twin
        ).wait_recv()

    def added(h, first, others, store):
        def strip(n, carry):
            at = pl.multiple_of(n * 16, 16)
            value = first(at).astype(jnp.float32)
            for other in others:
                value = value + other(at).astype(jnp.float32)
            store(at, value)
            return carry

        lax.fori_loop(0, cuts[h][1] // 16, strip, 0)

    def back_at(origin, h):
        return lambda at: back[pl.ds(pl.multiple_of(origin * rows + cuts[h][0] + at, 16), 16), :]

    def slot_at(ref, slot, h):
        return lambda at: ref[slot, pl.ds(pl.multiple_of(cuts[h][0] + at, 16), 16), :]

    def to_back(origin, h):
        def store(at, value):
            back[pl.ds(pl.multiple_of(origin * rows + cuts[h][0] + at, 16), 16), :] = value.astype(
                jnp.bfloat16
            )

        return store

    def side_out(j):
        twin_in(zs + j)
        origin = device(order[j], 1 - col, core)
        for h in straight:
            added(h, back_at(origin, h), [slot_at(from_twin, zs + j, h)], to_back(origin, h))
            side_push(j, h)

    def side_push(j, h):
        origin = device(order[j], 1 - col, core)
        push(
            back.at[part(origin, h)], from_side.at[j, local(h)],
            side_send.at[j, h], side_recv.at[j, h], side,
        )

    def side_in(j, h):
        view = from_side.at[j, local(h)]
        remote(view, view, side_send.at[j, h], side_recv.at[j, h], side).wait_recv()

    def far_in(ref, recv, slot, h):
        view = ref.at[slot, local(h)]
        remote(view, view, far_send.at[0, h], recv.at[slot, h], side).wait_recv()

    def chain(j, lane, ref, send, recv, label, h, extra):
        goal = order[j]
        origin = device(goal, lane, core)
        nearer = jnp.where(goal < level, level - 1, level + 1)
        behind = jnp.where(goal < level, level + 1, level - 1)
        slot = jnp.where((nearer == goal) & (goal > level), zs, goal)
        terms = [slot_at(from_twin, label, h)] + extra

        @pl.when((behind >= 0) & (behind < zs))
        def _():
            far_in(ref, recv, goal, h)
            added(h, back_at(origin, h), terms + [slot_at(ref, goal, h)], to_back(origin, h))

        @pl.when((behind < 0) | (behind >= zs))
        def _():
            added(h, back_at(origin, h), terms, to_back(origin, h))

        push(
            back.at[part(origin, h)], ref.at[slot, local(h)],
            send.at[j, h], recv.at[slot, h], device(nearer, col, core),
        )

    def gather_far(h, ref, recv):
        @pl.when(level > 0)
        def _():
            far_in(ref, recv, zs, h)
            added(h, total_at(h), [slot_at(ref, zs, h)], to_total(h))

        @pl.when(level < zs - 1)
        def _():
            far_in(ref, recv, level, h)
            added(h, total_at(h), [slot_at(ref, level, h)], to_total(h))

    def to_total(h):
        def store(at, value):
            total[pl.ds(pl.multiple_of(cuts[h][0] + at, 16), 16), :] = value

        return store

    def total_at(h):
        return lambda at: total[pl.ds(pl.multiple_of(cuts[h][0] + at, 16), 16), :]

    side_out(2)
    across_in(3)
    across_chip(3)
    for j in (3, 1, 0):
        side_out(j)

    for j in (2, 3, 1):
        chain(j, 1 - col, from_bent, bent_far_send, bent_far_recv, zs + j, bent, [])
    origin = device(level, 1 - col, core)
    added(bent, back_at(origin, bent), [slot_at(from_twin, zs, bent)], to_total(bent))
    gather_far(bent, from_bent, bent_far_recv)
    added(bent, total_at(bent), [], to_back(origin, bent))
    side_push(0, bent)

    for j in (2, 3, 1):
        twin_in(j)
        chain(j, col, from_far, far_send, far_recv, j, bent, [])
        for h in straight:
            side_in(j, h)
            chain(j, col, from_far, far_send, far_recv, j, h, [slot_at(from_side, j, h)])
    twin_in(0)
    for h in range(pieces):
        side_in(0, h)
        terms = [slot_at(from_twin, 0, h), slot_at(from_side, 0, h)]
        added(h, back_at(me, h), terms, to_total(h))
        gather_far(h, from_far, far_recv)

        def plain(ref):
            return lambda at: ref[pl.ds(pl.multiple_of(cuts[h][0] + at, 16), 16), :]

        def to_out(at, value):
            out[pl.ds(pl.multiple_of(cuts[h][0] + at, 16), 16), :] = value.astype(jnp.bfloat16)

        added(h, plain(middle), [total_at(h), plain(shared)], to_out)

    for j in range(zs):
        moves, to_twin = bent_copies(j)
        for allowed, copy in moves:
            pl.when(allowed)(copy.wait_send)
        to_twin.wait_send()
    for copy in sent:
        copy.wait_send()
    for h in range(pieces):
        piece = local(h)

        @pl.when(level > 0)
        def _():
            row_copy(own, piece, me, h, own_z_send.at[0, h], twin).wait_send()

        @pl.when(level < zs - 1)
        def _():
            row_copy(own, piece, me, h, own_z_send.at[1, h], twin).wait_send()

        for j in range(1, zs):
            for copy in fwd_copies(j, h):
                copy.wait_send()
            onward = onward_of(j)

            @pl.when((onward >= 0) & (onward < zs))
            def _():
                row_copy(own, piece, me, h, fwd_z_send.at[j, h], twin).wait_send()


def expert_stage(
    second_normed, middle, routes, route_weights,
    expert_gate, expert_up, expert_down, shared_gate, shared_up, shared_down,
):
    experts = lax.axis_size("ep")
    grid_shape = (experts // 4, 2, 2)
    zs = grid_shape[0]
    rows, width = second_normed.shape
    hid = expert_gate.shape[2]
    small = max(16, rows // 6 // 16 * 16)
    first = (rows - small) // 32 * 16 + (rows - small) // 16 % 2 * 16
    cuts = ((0, first), (first, rows - small - first), (rows - small, small))
    pieces = len(cuts)
    chosen = routes[None, :, :] == jnp.arange(experts, dtype=jnp.int32)[:, None, None]
    weights = jnp.sum(jnp.where(chosen, route_weights[None], 0.0), axis=2)
    weights = jnp.pad(weights, ((0, 0), (0, 128 - rows)))[:, None, :]
    vmem = pl.BlockSpec(memory_space=pltpu.VMEM)
    hbm = pl.BlockSpec(memory_space=pl.ANY)
    dma = pltpu.SemaphoreType.DMA
    half = jnp.bfloat16
    return pl.pallas_call(
        functools.partial(expert_kernel, grid_shape, cuts),
        out_shape=jax.ShapeDtypeStruct((rows, width), half),
        in_specs=[vmem] * 3 + [hbm] * 6,
        out_specs=vmem,
        scratch_shapes=[
            pltpu.VMEM((experts * rows, width), half),
            pltpu.VMEM((experts * rows, width), half),
            pltpu.VMEM((2 * zs, rows, width), half),
            pltpu.VMEM((zs, rows, width), half),
            pltpu.VMEM((zs + 1, rows, width), half),
            pltpu.VMEM((zs + 1, rows, width), half),
            pltpu.VMEM((experts, 1, 128), jnp.float32),
            pltpu.VMEM((width, hid), half),
            pltpu.VMEM((width, hid), half),
            pltpu.VMEM((hid, width), half),
            pltpu.VMEM(shared_gate.shape, half),
            pltpu.VMEM(shared_up.shape, half),
            pltpu.VMEM(shared_down.shape, half),
            pltpu.VMEM((2 * rows, hid), half),
            pltpu.VMEM((rows, width), half),
            pltpu.VMEM((rows, width), jnp.float32),
            dma((6,)),
            dma((experts, pieces)),
            dma((2, pieces)),
            dma((zs, pieces)),
            dma((zs, pieces)),
            dma((2 * zs, pieces)),
            dma((experts,)),
            dma((experts,)),
            dma((2 * zs,)),
            dma((2 * zs,)),
            dma((zs, pieces)),
            dma((zs, pieces)),
            dma((zs, pieces)),
            dma((zs + 1, pieces)),
            dma((zs + 1,)),
            dma((zs, pieces)),
            dma((zs + 1, pieces)),
        ],
        compiler_params=pltpu.CompilerParams(
            collective_id=0, has_side_effects=True, vmem_limit_bytes=60 * 1024 * 1024
        ),
    )(
        second_normed, middle, weights,
        expert_gate, expert_up, expert_down, shared_gate, shared_up, shared_down,
    )


def mixer_kernel(
    tokens, prior, mix_gain, in_weight, params, input_map, output_map, skip, out_weight,
    channel_gain, new_state, middle, second, normed, acts, acc,
):
    step = pl.program_id(0)
    lane = 128
    channels = in_weight.shape[1]
    width = input_map.shape[2]
    group = acts.shape[1] * width // prior.shape[2]
    per = lane // group
    states = per * width

    def scaled(values, gain):
        factor = lax.rsqrt(jnp.mean(values * values, axis=-1, keepdims=True) + norm_eps)
        return (values * factor * gain[...]).astype(jnp.bfloat16)

    @pl.when(step == 0)
    def _():
        normed[...] = scaled(tokens[...].astype(jnp.float32), mix_gain)
        acc[...] = jnp.zeros_like(acc)

    drive = jnp.dot(normed[...], in_weight[...], preferred_element_type=jnp.float32)
    drive = drive.astype(jnp.bfloat16)
    row = lax.broadcasted_iota(jnp.int32, (lane, states), 0) // group
    column = lax.broadcasted_iota(jnp.int32, (lane, states), 1) // width
    own_group = row == column

    def spread(table):
        tiled = jnp.concatenate([table] * per, axis=1)
        return jnp.where(own_group, tiled, 0.0).astype(jnp.bfloat16)

    for sub in range(channels // lane):
        cols = slice(sub * lane, (sub + 1) * lane)
        ent = slice(sub * states, (sub + 1) * states)
        part = drive[:, cols]
        push_real = jnp.dot(
            part, spread(input_map[0, cols, :]), preferred_element_type=jnp.float32
        )
        push_imag = jnp.dot(
            part, spread(input_map[1, cols, :]), preferred_element_type=jnp.float32
        )
        turn_real, turn_imag = params[0:1, ent], params[1:2, ent]
        hold_real, hold_imag = params[2:3, ent], params[3:4, ent]
        old_real, old_imag = prior[0, :, ent], prior[1, :, ent]
        fresh_real = (
            turn_real * old_real - turn_imag * old_imag
            + (push_real * hold_real - push_imag * hold_imag)
        )
        fresh_imag = (
            turn_real * old_imag + turn_imag * old_real
            + (push_real * hold_imag + push_imag * hold_real)
        )
        new_state[0, :, ent] = fresh_real
        new_state[1, :, ent] = fresh_imag
        across = (((1,), (1,)), ((), ()))
        readout = lax.dot_general(
            fresh_real.astype(jnp.bfloat16), spread(output_map[0, cols, :]), across,
            preferred_element_type=jnp.float32,
        ) - lax.dot_general(
            fresh_imag.astype(jnp.bfloat16), spread(output_map[1, cols, :]), across,
            preferred_element_type=jnp.float32,
        )
        readout = readout + skip[:, cols] * part.astype(jnp.float32)
        acts[:, cols] = jax.nn.gelu(readout).astype(jnp.bfloat16)
    acc[...] += jnp.dot(acts[...], out_weight[...], preferred_element_type=jnp.float32)

    @pl.when(step == pl.num_programs(0) - 1)
    def _():
        mixed = acc[...].astype(jnp.bfloat16).astype(jnp.float32)
        mid = (tokens[...].astype(jnp.float32) + mixed).astype(jnp.bfloat16)
        middle[...] = mid
        second[...] = scaled(mid.astype(jnp.float32), channel_gain)


def mixer_stage(
    tokens, prior_state, mix_gain, in_weight, decay_rate, frequency, log_step,
    input_map, output_map, skip_gain, out_weight, channel_gain,
):
    rows, model = tokens.shape
    groups, width = decay_rate.shape
    channels = in_weight.shape[1]
    step_size = jnp.exp(log_step)[:, None]
    real_rate = -decay_rate
    magnitude = jnp.exp(real_rate * step_size)
    turn_real = magnitude * jnp.cos(frequency * step_size)
    turn_imag = magnitude * jnp.sin(frequency * step_size)
    denominator = real_rate * real_rate + frequency * frequency
    hold_real = ((turn_real - 1.0) * real_rate + turn_imag * frequency) / denominator
    hold_imag = (turn_imag * real_rate - (turn_real - 1.0) * frequency) / denominator
    params = jnp.stack([turn_real, turn_imag, hold_real, hold_imag]).reshape(4, -1)
    in_map = jnp.transpose(input_map, (0, 1, 3, 2)).reshape(2, channels, width)
    out_map = output_map.reshape(2, channels, width)
    block = 256
    states = block * groups * width // channels

    def whole(*shape):
        return pl.BlockSpec(shape, lambda i: (0,) * len(shape))

    half = jnp.bfloat16
    return pl.pallas_call(
        mixer_kernel,
        grid=(channels // block,),
        out_shape=(
            jax.ShapeDtypeStruct(prior_state.shape, jnp.float32),
            jax.ShapeDtypeStruct((rows, model), half),
            jax.ShapeDtypeStruct((rows, model), half),
        ),
        in_specs=[
            whole(rows, model),
            pl.BlockSpec((2, rows, states), lambda i: (0, 0, i)),
            whole(1, model),
            pl.BlockSpec((model, block), lambda i: (0, i)),
            pl.BlockSpec((4, states), lambda i: (0, i)),
            pl.BlockSpec((2, block, width), lambda i: (0, i, 0)),
            pl.BlockSpec((2, block, width), lambda i: (0, i, 0)),
            pl.BlockSpec((1, block), lambda i: (0, i)),
            pl.BlockSpec((block, model), lambda i: (i, 0)),
            whole(1, model),
        ],
        out_specs=(
            pl.BlockSpec((2, rows, states), lambda i: (0, 0, i)),
            whole(rows, model),
            whole(rows, model),
        ),
        scratch_shapes=[
            pltpu.VMEM((rows, model), half),
            pltpu.VMEM((rows, block), half),
            pltpu.VMEM((rows, model), jnp.float32),
        ],
        compiler_params=pltpu.CompilerParams(
            dimension_semantics=("arbitrary",), vmem_limit_bytes=62 * 1024 * 1024
        ),
    )(
        tokens, prior_state, mix_gain[None], in_weight, params, in_map, out_map,
        skip_gain[None], out_weight, channel_gain[None],
    )


def body(
    tokens,
    prior_state,
    mix_gain,
    in_weight,
    decay_rate,
    frequency,
    log_step,
    input_map,
    output_map,
    skip_gain,
    out_weight,
    channel_gain,
    expert_gate,
    expert_up,
    expert_down,
    shared_gate,
    shared_up,
    shared_down,
    routes,
    route_weights,
):
    if lax.axis_size("tp") == 1 and lax.axis_size("ep") == 16:
        new_state, middle, second_normed = mixer_stage(
            tokens, prior_state, mix_gain, in_weight, decay_rate, frequency, log_step,
            input_map, output_map, skip_gain, out_weight, channel_gain,
        )
        layer_out = expert_stage(
            second_normed, middle, routes, route_weights,
            expert_gate, expert_up, expert_down, shared_gate, shared_up, shared_down,
        )
        return (layer_out, new_state)
    normed = root_scale(tokens, mix_gain)
    drive_rows = jnp.dot(normed, in_weight, preferred_element_type=jnp.float32).astype(jnp.bfloat16)
    readout, new_state = state_update(
        drive_rows, prior_state, decay_rate, frequency, log_step, input_map, output_map, skip_gain
    )
    activated = jax.nn.gelu(readout).astype(jnp.bfloat16)
    partial_value = jnp.dot(activated, out_weight, preferred_element_type=jnp.float32)
    mixer_out = lax.psum(partial_value.astype(jnp.bfloat16), "tp").astype(jnp.float32)
    middle = (tokens.astype(jnp.float32) + mixer_out).astype(jnp.bfloat16)
    second_normed = root_scale(middle, channel_gain)
    shared_gval = jnp.dot(second_normed, shared_gate, preferred_element_type=jnp.float32)
    shared_uval = jnp.dot(second_normed, shared_up, preferred_element_type=jnp.float32)
    shared_hidden = (jax.nn.silu(shared_gval) * shared_uval).astype(jnp.bfloat16)
    shared_piece = jnp.dot(shared_hidden, shared_down, preferred_element_type=jnp.float32)
    shared_out = lax.psum_scatter(
        shared_piece.astype(jnp.bfloat16), "tp", scatter_dimension=1, tiled=True
    ).astype(jnp.float32)
    half_cols = second_normed.shape[1] // lax.axis_size("tp")
    routed = exchanged_experts(
        second_normed, routes, route_weights, expert_gate, expert_up, expert_down
    )
    own_middle = lax.dynamic_slice_in_dim(middle, lax.axis_index("tp") * half_cols, half_cols, 1)
    layer_out = (own_middle.astype(jnp.float32) + routed + shared_out).astype(jnp.bfloat16)
    return (layer_out, new_state)


def solution(mesh):
    in_specs = (
        P(("grp", "ep"), None),
        P(None, ("grp", "ep"), "tp"),
        P(),
        P(None, "tp"),
        P("tp", None),
        P("tp", None),
        P("tp"),
        P(None, "tp", None, None),
        P(None, "tp", None, None),
        P("tp"),
        P("tp", None),
        P(),
        P("ep", None, "tp"),
        P("ep", None, "tp"),
        P("ep", "tp", None),
        P(None, "tp"),
        P(None, "tp"),
        P("tp", None),
        P(("grp", "ep"), None),
        P(("grp", "ep"), None),
    )
    out_specs = (P(("grp", "ep"), "tp"), P(None, ("grp", "ep"), "tp"))
    return jax.shard_map(body, mesh=mesh, in_specs=in_specs, out_specs=out_specs, check_vma=False)
```

```python
import functools
import jax
import jax.numpy as jnp
from jax import lax
from jax.experimental import pallas as pl
from jax.experimental.pallas import tpu as pltpu
from jax.sharding import PartitionSpec as P

norm_eps = 1e-06
highest = lax.Precision.HIGHEST
MESH = pl.DeviceIdType.MESH


def root_scale(activations, scale_gain):
    values = activations.astype(jnp.float32)
    factor = lax.rsqrt(jnp.mean(values * values, axis=-1, keepdims=True) + norm_eps)
    return (values * factor * scale_gain).astype(jnp.bfloat16)


def state_update(
    drive_rows, prior_state, decay_rate, frequency, log_step, input_map, output_map, skip_gain
):
    sequences = drive_rows.shape[0]
    groups = decay_rate.shape[0]
    driven = drive_rows.astype(jnp.float32).reshape(sequences, groups, -1)
    step_size = jnp.exp(log_step)[:, None]
    real_rate = -decay_rate
    magnitude = jnp.exp(real_rate * step_size)
    turn_real = magnitude * jnp.cos(frequency * step_size)
    turn_imag = magnitude * jnp.sin(frequency * step_size)
    denominator = real_rate * real_rate + frequency * frequency
    hold_real = ((turn_real - 1.0) * real_rate + turn_imag * frequency) / denominator
    hold_imag = (turn_imag * real_rate - (turn_real - 1.0) * frequency) / denominator
    push_real = jnp.einsum("sgh,gph->sgp", driven, input_map[0], precision=highest)
    push_imag = jnp.einsum("sgh,gph->sgp", driven, input_map[1], precision=highest)
    enter_real = push_real * hold_real - push_imag * hold_imag
    enter_imag = push_real * hold_imag + push_imag * hold_real
    old_real = prior_state[0].reshape(sequences, groups, -1)
    old_imag = prior_state[1].reshape(sequences, groups, -1)
    fresh_real = turn_real * old_real - turn_imag * old_imag + enter_real
    fresh_imag = turn_real * old_imag + turn_imag * old_real + enter_imag
    readout = jnp.einsum("ghp,sgp->sgh", output_map[0], fresh_real, precision=highest)
    readout = readout - jnp.einsum("ghp,sgp->sgh", output_map[1], fresh_imag, precision=highest)
    readout = readout.reshape(sequences, -1) + skip_gain * drive_rows.astype(jnp.float32)
    fresh = jnp.stack([fresh_real.reshape(sequences, -1), fresh_imag.reshape(sequences, -1)])
    return (readout, fresh)


def exchanged_experts(second_normed, routes, route_weights, expert_gate, expert_up, expert_down):
    experts = lax.axis_size("ep")
    seq_rows, top_count = routes.shape
    slot_cap = min(seq_rows, max(2, 3 * seq_rows * top_count // (2 * experts)))
    flat_routes = routes.reshape(-1)
    one_hot = (flat_routes[:, None] == jnp.arange(experts, dtype=jnp.int32)[None, :]).astype(
        jnp.int32
    )
    ranked = jnp.sum((jnp.cumsum(one_hot, axis=0) - one_hot) * one_hot, axis=1)
    slot_index = flat_routes * slot_cap + ranked
    placed = slot_index[:, None] == jnp.arange(experts * slot_cap, dtype=jnp.int32)[None, :]
    placed_rows = jnp.any(placed.reshape(seq_rows, top_count, experts * slot_cap), axis=1).astype(
        jnp.bfloat16
    )
    outgoing = lax.dot_general(
        placed_rows, second_normed, (((0,), (0,)), ((), ())), preferred_element_type=jnp.float32
    ).astype(jnp.bfloat16)
    outgoing = outgoing.reshape(experts, slot_cap, -1)
    arrived = lax.all_to_all(outgoing, "ep", split_axis=0, concat_axis=0, tiled=True)
    sources, count_items, full_width = arrived.shape
    expert_rows = arrived.reshape(sources * count_items, full_width)
    gate_val = jnp.dot(expert_rows, expert_gate[0], preferred_element_type=jnp.float32)
    up_val = jnp.dot(expert_rows, expert_up[0], preferred_element_type=jnp.float32)
    hidden = (jax.nn.silu(gate_val) * up_val).astype(jnp.bfloat16)
    piece = jnp.dot(hidden, expert_down[0], preferred_element_type=jnp.float32)
    summed = lax.psum_scatter(
        piece.reshape(sources, count_items, full_width).astype(jnp.bfloat16),
        "tp",
        scatter_dimension=2,
        tiled=True,
    )
    returned = lax.all_to_all(summed, "ep", split_axis=0, concat_axis=0, tiled=True)
    flat_back = returned.reshape(experts * slot_cap, -1)
    picked = (
        jnp.take(flat_back, slot_index, axis=0).reshape(seq_rows, top_count, -1).astype(jnp.float32)
    )
    routed = jnp.einsum("sk,skd->sd", route_weights, picked)
    return routed


def near_first(extent):
    return [sorted(range(extent), key=lambda other: (abs(other - at), min(other, extent - 1 - other))) for at in range(extent)]


def looked_up(table, position):
    found = jnp.int32(0)
    for at, entry in enumerate(table):
        found = jnp.where(position == at, jnp.int32(entry), found)
    return found


def expert_kernel(
    grid_shape, pieces,
    own, middle, weights, gate_in, up_in, down_in, sgate_in, sup_in, sdown_in,
    out,
    rows_all, back, from_twin, from_side, from_far, weight_all,
    gate, up, down, sgate, sup, sdown, hidden, shared, total,
    load_sem, row_recv, own_z_send, fwd_z_send, fwd_x_send, fwd_twin_send,
    w_send, w_recv, twin_send, twin_recv, side_send, side_recv, far_send, far_recv,
):
    zs, xs, cs = grid_shape
    count = zs * xs * cs
    me = lax.axis_index("ep")
    core = lax.rem(me, cs)
    col = lax.rem(me // cs, xs)
    level = me // (cs * xs)
    rows, width = own.shape
    span = rows // pieces
    hid = gate.shape[1]

    def device(z, x, c):
        return (z * xs + x) * cs + c

    twin = device(level, col, 1 - core)
    side = device(level, 1 - col, core)
    order = [looked_up([row[j] for row in near_first(zs)], level) for j in range(zs)]

    def part(base, h):
        return pl.ds(pl.multiple_of(base * rows + h * span, 16), span)

    loads = [
        pltpu.make_async_copy(src, dst, load_sem.at[n])
        for n, (src, dst) in enumerate(
            ((gate_in.at[0], gate), (up_in.at[0], up), (down_in.at[0], down),
             (sgate_in, sgate), (sup_in, sup), (sdown_in, sdown))
        )
    ]
    for load in loads:
        load.start()

    barrier = pltpu.get_barrier_semaphore()
    for step in range(1, count):
        pl.semaphore_signal(
            barrier, inc=1, device_id={"ep": lax.rem(me + step, count)}, device_id_type=MESH
        )
    pl.semaphore_wait(barrier, count - 1)

    def remote(src, dst, send, recv, target):
        return pltpu.make_async_remote_copy(
            src_ref=src, dst_ref=dst, send_sem=send, recv_sem=recv,
            device_id={"ep": target}, device_id_type=MESH,
        )

    sent = []

    def push(src, dst, send, recv, target):
        copy = remote(src, dst, send, recv, target)
        copy.start()
        sent.append(copy)

    def row_copy(src_ref, src_rows, origin, h, send, target):
        return remote(
            src_ref.at[src_rows], rows_all.at[part(origin, h)], send, row_recv.at[origin, h], target
        )

    for h in range(pieces):
        piece = pl.ds(h * span, span)

        @pl.when(level > 0)
        def _():
            row_copy(own, piece, me, h, own_z_send.at[0, h], device(level - 1, col, core)).start()

        @pl.when(level < zs - 1)
        def _():
            row_copy(own, piece, me, h, own_z_send.at[1, h], device(level + 1, col, core)).start()

        for send, target in ((fwd_x_send.at[0, h], side), (fwd_twin_send.at[0, h], twin)):
            copy = row_copy(own, piece, me, h, send, target)
            copy.start()
            sent.append(copy)

    for step in range(1, count):
        other = lax.rem(me + step, count)
        push(
            weights.at[other], weight_all.at[me], w_send.at[step], w_recv.at[count - step], other
        )
    rows_all[part(me, 0), :] = own[pl.ds(0, span), :]
    for h in range(1, pieces):
        rows_all[part(me, h), :] = own[pl.ds(h * span, span), :]
    weight_all[me] = weights[me]

    def arrived(origin, h):
        row_copy(own, pl.ds(h * span, span), origin, h, own_z_send.at[0, h], twin).wait_recv()

    def feed(source, take, gate_w, up_w, down_w, finish):
        def first(n, carry):
            cols = pl.ds(pl.multiple_of(n * 256, 256), 256)
            data = source()
            g = jnp.dot(data, gate_w[:, cols], preferred_element_type=jnp.float32)
            u = jnp.dot(data, up_w[:, cols], preferred_element_type=jnp.float32)
            hidden[pl.ds(0, take), cols] = (jax.nn.silu(g) * u).astype(jnp.bfloat16)
            return carry

        lax.fori_loop(0, hid // 256, first, 0)

        def second(n, carry):
            cols = pl.ds(pl.multiple_of(n * 512, 512), 512)
            piece = jnp.dot(
                hidden[pl.ds(0, take), :], down_w[:, cols], preferred_element_type=jnp.float32
            )
            finish(cols, piece.astype(jnp.bfloat16))
            return carry

        lax.fori_loop(0, width // 512, second, 0)

    def chip(label, z, x):
        base = device(z, x, 0)
        block = pl.ds(pl.multiple_of(base * rows, 16), cs * rows)
        scales = []
        for c in range(cs):
            line = jnp.broadcast_to(weight_all[base + c], (128, 128))
            scales.append(jnp.transpose(line)[:rows])
        scale = jnp.concatenate(scales, axis=0)
        scale = jnp.concatenate([scale] * 4, axis=1)

        def finish(cols, piece):
            back[block, cols] = (piece.astype(jnp.float32) * scale).astype(jnp.bfloat16)

        feed(lambda: rows_all[block, :], cs * rows, gate, up, down, finish)
        push(
            back.at[part_all(device(z, x, 1 - core))],
            from_twin.at[label],
            twin_send.at[label],
            twin_recv.at[label],
            twin,
        )

    def part_all(origin):
        return pl.ds(pl.multiple_of(origin * rows, 16), rows)

    def keep(cols, piece):
        shared[:, cols] = piece

    def pair_in(z, x):
        for h in range(pieces):
            arrived(device(z, x, 1 - core), h)

    def onward_of(j):
        return jnp.where(order[j] < level, level + 1, level - 1)

    def fwd_copies(j, h):
        origin = device(order[j], col, core)
        return [
            row_copy(rows_all, part(origin, h), origin, h, send, target)
            for send, target in ((fwd_x_send.at[j, h], side), (fwd_twin_send.at[j, h], twin))
        ]

    def fwd(j):
        for h in range(pieces):
            fwd_piece(j, h)

    def fwd_piece(j, h):
        origin = device(order[j], col, core)
        arrived(origin, h)
        onward = onward_of(j)

        @pl.when((onward >= 0) & (onward < zs))
        def _():
            row_copy(
                rows_all, part(origin, h), origin, h, fwd_z_send.at[j, h],
                device(onward, col, core),
            ).start()

        for copy in fwd_copies(j, h):
            copy.start()

    def across_in(j):
        across = device(order[j], 1 - col, core)
        for h in range(pieces):
            arrived(across, h)
            copy = row_copy(rows_all, part(across, h), across, h, fwd_twin_send.at[zs + j, h], twin)
            copy.start()
            sent.append(copy)

    def own_chip(j):
        pair_in(order[j], col)
        chip(j, order[j], col)

    def across_chip(j):
        pair_in(order[j], 1 - col)
        chip(zs + j, order[j], 1 - col)

    inner = (level > 0) & (level < zs - 1)
    outer = (level == 0) | (level == zs - 1)

    for load in loads[:3]:
        load.wait()
    for step in range(1, count):
        remote(
            weights.at[me], weight_all.at[lax.rem(me + step, count)],
            w_send.at[step], w_recv.at[step], twin,
        ).wait_recv()
    own_chip(0)
    for h in range(pieces):
        fwd_piece(1, h)
        pl.when(inner)(functools.partial(fwd_piece, 2, h))
        if h == 0:
            for load in loads[3:]:
                load.wait()
            feed(lambda: own[...], rows, sgate, sup, sdown, keep)
    across_in(0)
    own_chip(1)
    across_chip(0)
    for h in range(pieces):
        pl.when(inner)(functools.partial(fwd_piece, 3, h))
        pl.when(outer)(functools.partial(fwd_piece, 2, h))
    across_in(1)
    own_chip(2)
    across_chip(1)
    pl.when(outer)(functools.partial(fwd, 3))
    across_in(2)
    own_chip(3)
    across_chip(2)

    def twin_in(label):
        remote(
            from_twin.at[label], from_twin.at[label], twin_send.at[label], twin_recv.at[label], twin
        ).wait_recv()

    def added(first, others, store):
        def strip(n, carry):
            at = pl.multiple_of(n * 16, 16)
            value = first(at).astype(jnp.float32)
            for other in others:
                value = value + other(at).astype(jnp.float32)
            store(at, value)
            return carry

        lax.fori_loop(0, span // 16, strip, 0)

    def back_at(origin, h):
        return lambda at: back[pl.ds(pl.multiple_of(origin * rows + h * span + at, 16), 16), :]

    def slot_at(ref, slot, h):
        return lambda at: ref[slot, pl.ds(pl.multiple_of(h * span + at, 16), 16), :]

    def to_back(origin, h):
        def store(at, value):
            back[pl.ds(pl.multiple_of(origin * rows + h * span + at, 16), 16), :] = value.astype(
                jnp.bfloat16
            )

        return store

    def side_out(j):
        twin_in(zs + j)
        origin = device(order[j], 1 - col, core)
        for h in range(pieces):
            added(back_at(origin, h), [slot_at(from_twin, zs + j, h)], to_back(origin, h))
            push(
                back.at[part(origin, h)], from_side.at[j, pl.ds(h * span, span)],
                side_send.at[j, h], side_recv.at[j, h], side,
            )

    side_out(2)
    across_in(3)
    across_chip(3)
    for j in (3, 1, 0):
        side_out(j)

    def side_in(j, h):
        view = from_side.at[j, pl.ds(h * span, span)]
        remote(view, view, side_send.at[j, h], side_recv.at[j, h], side).wait_recv()

    def far_in(slot, h):
        view = from_far.at[slot, pl.ds(h * span, span)]
        remote(view, view, far_send.at[0, h], far_recv.at[slot, h], side).wait_recv()

    for j in (2, 3, 1):
        twin_in(j)
        goal = order[j]
        origin = device(goal, col, core)
        nearer = jnp.where(goal < level, level - 1, level + 1)
        behind = jnp.where(goal < level, level + 1, level - 1)
        slot = jnp.where((nearer == goal) & (goal > level), zs, goal)
        for h in range(pieces):
            side_in(j, h)
            terms = [slot_at(from_twin, j, h), slot_at(from_side, j, h)]

            @pl.when((behind >= 0) & (behind < zs))
            def _():
                far_in(goal, h)
                added(
                    back_at(origin, h), terms + [slot_at(from_far, goal, h)], to_back(origin, h)
                )

            @pl.when((behind < 0) | (behind >= zs))
            def _():
                added(back_at(origin, h), terms, to_back(origin, h))

            push(
                back.at[part(origin, h)], from_far.at[slot, pl.ds(h * span, span)],
                far_send.at[j, h], far_recv.at[slot, h], device(nearer, col, core),
            )
    twin_in(0)
    for h in range(pieces):
        side_in(0, h)

        def to_total(at, value):
            total[pl.ds(pl.multiple_of(h * span + at, 16), 16), :] = value

        def total_at(at):
            return total[pl.ds(pl.multiple_of(h * span + at, 16), 16), :]

        added(back_at(me, h), [slot_at(from_twin, 0, h), slot_at(from_side, 0, h)], to_total)

        @pl.when(level > 0)
        def _():
            far_in(zs, h)
            added(total_at, [slot_at(from_far, zs, h)], to_total)

        @pl.when(level < zs - 1)
        def _():
            far_in(level, h)
            added(total_at, [slot_at(from_far, level, h)], to_total)

        def plain(ref):
            return lambda at: ref[pl.ds(pl.multiple_of(h * span + at, 16), 16), :]

        def to_out(at, value):
            out[pl.ds(pl.multiple_of(h * span + at, 16), 16), :] = value.astype(jnp.bfloat16)

        added(plain(middle), [total_at, plain(shared)], to_out)

    for copy in sent:
        copy.wait_send()
    for h in range(pieces):
        piece = pl.ds(h * span, span)

        @pl.when(level > 0)
        def _():
            row_copy(own, piece, me, h, own_z_send.at[0, h], twin).wait_send()

        @pl.when(level < zs - 1)
        def _():
            row_copy(own, piece, me, h, own_z_send.at[1, h], twin).wait_send()

        for j in range(1, zs):
            for copy in fwd_copies(j, h):
                copy.wait_send()
            onward = onward_of(j)

            @pl.when((onward >= 0) & (onward < zs))
            def _():
                row_copy(own, piece, me, h, fwd_z_send.at[j, h], twin).wait_send()


def expert_stage(
    second_normed, middle, routes, route_weights,
    expert_gate, expert_up, expert_down, shared_gate, shared_up, shared_down,
):
    experts = lax.axis_size("ep")
    grid_shape = (experts // 4, 2, 2)
    zs = grid_shape[0]
    rows, width = second_normed.shape
    hid = expert_gate.shape[2]
    pieces = 3 if rows % 48 == 0 else 1
    chosen = routes[None, :, :] == jnp.arange(experts, dtype=jnp.int32)[:, None, None]
    weights = jnp.sum(jnp.where(chosen, route_weights[None], 0.0), axis=2)
    weights = jnp.pad(weights, ((0, 0), (0, 128 - rows)))[:, None, :]
    vmem = pl.BlockSpec(memory_space=pltpu.VMEM)
    hbm = pl.BlockSpec(memory_space=pl.ANY)
    dma = pltpu.SemaphoreType.DMA
    half = jnp.bfloat16
    return pl.pallas_call(
        functools.partial(expert_kernel, grid_shape, pieces),
        out_shape=jax.ShapeDtypeStruct((rows, width), half),
        in_specs=[vmem] * 3 + [hbm] * 6,
        out_specs=vmem,
        scratch_shapes=[
            pltpu.VMEM((experts * rows, width), half),
            pltpu.VMEM((experts * rows, width), half),
            pltpu.VMEM((2 * zs, rows, width), half),
            pltpu.VMEM((zs, rows, width), half),
            pltpu.VMEM((zs + 1, rows, width), half),
            pltpu.VMEM((experts, 1, 128), jnp.float32),
            pltpu.VMEM((width, hid), half),
            pltpu.VMEM((width, hid), half),
            pltpu.VMEM((hid, width), half),
            pltpu.VMEM(shared_gate.shape, half),
            pltpu.VMEM(shared_up.shape, half),
            pltpu.VMEM(shared_down.shape, half),
            pltpu.VMEM((2 * rows, hid), half),
            pltpu.VMEM((rows, width), half),
            pltpu.VMEM((rows, width), jnp.float32),
            dma((6,)),
            dma((experts, pieces)),
            dma((2, pieces)),
            dma((zs, pieces)),
            dma((zs, pieces)),
            dma((2 * zs, pieces)),
            dma((experts,)),
            dma((experts,)),
            dma((2 * zs,)),
            dma((2 * zs,)),
            dma((zs, pieces)),
            dma((zs, pieces)),
            dma((zs, pieces)),
            dma((zs + 1, pieces)),
        ],
        compiler_params=pltpu.CompilerParams(
            collective_id=0, has_side_effects=True, vmem_limit_bytes=60 * 1024 * 1024
        ),
    )(
        second_normed, middle, weights,
        expert_gate, expert_up, expert_down, shared_gate, shared_up, shared_down,
    )


def mixer_kernel(
    tokens, prior, mix_gain, in_weight, params, input_map, output_map, skip, out_weight,
    channel_gain, new_state, middle, second, normed, acts, acc,
):
    step = pl.program_id(0)
    lane = 128
    channels = in_weight.shape[1]
    width = input_map.shape[2]
    group = acts.shape[1] * width // prior.shape[2]
    per = lane // group
    states = per * width

    def scaled(values, gain):
        factor = lax.rsqrt(jnp.mean(values * values, axis=-1, keepdims=True) + norm_eps)
        return (values * factor * gain[...]).astype(jnp.bfloat16)

    @pl.when(step == 0)
    def _():
        normed[...] = scaled(tokens[...].astype(jnp.float32), mix_gain)
        acc[...] = jnp.zeros_like(acc)

    drive = jnp.dot(normed[...], in_weight[...], preferred_element_type=jnp.float32)
    drive = drive.astype(jnp.bfloat16)
    row = lax.broadcasted_iota(jnp.int32, (lane, states), 0) // group
    column = lax.broadcasted_iota(jnp.int32, (lane, states), 1) // width
    own_group = row == column

    def spread(table):
        tiled = jnp.concatenate([table] * per, axis=1)
        return jnp.where(own_group, tiled, 0.0).astype(jnp.bfloat16)

    for sub in range(channels // lane):
        cols = slice(sub * lane, (sub + 1) * lane)
        ent = slice(sub * states, (sub + 1) * states)
        part = drive[:, cols]
        push_real = jnp.dot(
            part, spread(input_map[0, cols, :]), preferred_element_type=jnp.float32
        )
        push_imag = jnp.dot(
            part, spread(input_map[1, cols, :]), preferred_element_type=jnp.float32
        )
        turn_real, turn_imag = params[0:1, ent], params[1:2, ent]
        hold_real, hold_imag = params[2:3, ent], params[3:4, ent]
        old_real, old_imag = prior[0, :, ent], prior[1, :, ent]
        fresh_real = (
            turn_real * old_real - turn_imag * old_imag
            + (push_real * hold_real - push_imag * hold_imag)
        )
        fresh_imag = (
            turn_real * old_imag + turn_imag * old_real
            + (push_real * hold_imag + push_imag * hold_real)
        )
        new_state[0, :, ent] = fresh_real
        new_state[1, :, ent] = fresh_imag
        across = (((1,), (1,)), ((), ()))
        readout = lax.dot_general(
            fresh_real.astype(jnp.bfloat16), spread(output_map[0, cols, :]), across,
            preferred_element_type=jnp.float32,
        ) - lax.dot_general(
            fresh_imag.astype(jnp.bfloat16), spread(output_map[1, cols, :]), across,
            preferred_element_type=jnp.float32,
        )
        readout = readout + skip[:, cols] * part.astype(jnp.float32)
        acts[:, cols] = jax.nn.gelu(readout).astype(jnp.bfloat16)
    acc[...] += jnp.dot(acts[...], out_weight[...], preferred_element_type=jnp.float32)

    @pl.when(step == pl.num_programs(0) - 1)
    def _():
        mixed = acc[...].astype(jnp.bfloat16).astype(jnp.float32)
        mid = (tokens[...].astype(jnp.float32) + mixed).astype(jnp.bfloat16)
        middle[...] = mid
        second[...] = scaled(mid.astype(jnp.float32), channel_gain)


def mixer_stage(
    tokens, prior_state, mix_gain, in_weight, decay_rate, frequency, log_step,
    input_map, output_map, skip_gain, out_weight, channel_gain,
):
    rows, model = tokens.shape
    groups, width = decay_rate.shape
    channels = in_weight.shape[1]
    step_size = jnp.exp(log_step)[:, None]
    real_rate = -decay_rate
    magnitude = jnp.exp(real_rate * step_size)
    turn_real = magnitude * jnp.cos(frequency * step_size)
    turn_imag = magnitude * jnp.sin(frequency * step_size)
    denominator = real_rate * real_rate + frequency * frequency
    hold_real = ((turn_real - 1.0) * real_rate + turn_imag * frequency) / denominator
    hold_imag = (turn_imag * real_rate - (turn_real - 1.0) * frequency) / denominator
    params = jnp.stack([turn_real, turn_imag, hold_real, hold_imag]).reshape(4, -1)
    in_map = jnp.transpose(input_map, (0, 1, 3, 2)).reshape(2, channels, width)
    out_map = output_map.reshape(2, channels, width)
    block = 256
    states = block * groups * width // channels

    def whole(*shape):
        return pl.BlockSpec(shape, lambda i: (0,) * len(shape))

    half = jnp.bfloat16
    return pl.pallas_call(
        mixer_kernel,
        grid=(channels // block,),
        out_shape=(
            jax.ShapeDtypeStruct(prior_state.shape, jnp.float32),
            jax.ShapeDtypeStruct((rows, model), half),
            jax.ShapeDtypeStruct((rows, model), half),
        ),
        in_specs=[
            whole(rows, model),
            pl.BlockSpec((2, rows, states), lambda i: (0, 0, i)),
            whole(1, model),
            pl.BlockSpec((model, block), lambda i: (0, i)),
            pl.BlockSpec((4, states), lambda i: (0, i)),
            pl.BlockSpec((2, block, width), lambda i: (0, i, 0)),
            pl.BlockSpec((2, block, width), lambda i: (0, i, 0)),
            pl.BlockSpec((1, block), lambda i: (0, i)),
            pl.BlockSpec((block, model), lambda i: (i, 0)),
            whole(1, model),
        ],
        out_specs=(
            pl.BlockSpec((2, rows, states), lambda i: (0, 0, i)),
            whole(rows, model),
            whole(rows, model),
        ),
        scratch_shapes=[
            pltpu.VMEM((rows, model), half),
            pltpu.VMEM((rows, block), half),
            pltpu.VMEM((rows, model), jnp.float32),
        ],
        compiler_params=pltpu.CompilerParams(
            dimension_semantics=("arbitrary",), vmem_limit_bytes=62 * 1024 * 1024
        ),
    )(
        tokens, prior_state, mix_gain[None], in_weight, params, in_map, out_map,
        skip_gain[None], out_weight, channel_gain[None],
    )


def body(
    tokens,
    prior_state,
    mix_gain,
    in_weight,
    decay_rate,
    frequency,
    log_step,
    input_map,
    output_map,
    skip_gain,
    out_weight,
    channel_gain,
    expert_gate,
    expert_up,
    expert_down,
    shared_gate,
    shared_up,
    shared_down,
    routes,
    route_weights,
):
    if lax.axis_size("tp") == 1 and lax.axis_size("ep") == 16:
        new_state, middle, second_normed = mixer_stage(
            tokens, prior_state, mix_gain, in_weight, decay_rate, frequency, log_step,
            input_map, output_map, skip_gain, out_weight, channel_gain,
        )
        layer_out = expert_stage(
            second_normed, middle, routes, route_weights,
            expert_gate, expert_up, expert_down, shared_gate, shared_up, shared_down,
        )
        return (layer_out, new_state)
    normed = root_scale(tokens, mix_gain)
    drive_rows = jnp.dot(normed, in_weight, preferred_element_type=jnp.float32).astype(jnp.bfloat16)
    readout, new_state = state_update(
        drive_rows, prior_state, decay_rate, frequency, log_step, input_map, output_map, skip_gain
    )
    activated = jax.nn.gelu(readout).astype(jnp.bfloat16)
    partial_value = jnp.dot(activated, out_weight, preferred_element_type=jnp.float32)
    mixer_out = lax.psum(partial_value.astype(jnp.bfloat16), "tp").astype(jnp.float32)
    middle = (tokens.astype(jnp.float32) + mixer_out).astype(jnp.bfloat16)
    second_normed = root_scale(middle, channel_gain)
    shared_gval = jnp.dot(second_normed, shared_gate, preferred_element_type=jnp.float32)
    shared_uval = jnp.dot(second_normed, shared_up, preferred_element_type=jnp.float32)
    shared_hidden = (jax.nn.silu(shared_gval) * shared_uval).astype(jnp.bfloat16)
    shared_piece = jnp.dot(shared_hidden, shared_down, preferred_element_type=jnp.float32)
    shared_out = lax.psum_scatter(
        shared_piece.astype(jnp.bfloat16), "tp", scatter_dimension=1, tiled=True
    ).astype(jnp.float32)
    half_cols = second_normed.shape[1] // lax.axis_size("tp")
    routed = exchanged_experts(
        second_normed, routes, route_weights, expert_gate, expert_up, expert_down
    )
    own_middle = lax.dynamic_slice_in_dim(middle, lax.axis_index("tp") * half_cols, half_cols, 1)
    layer_out = (own_middle.astype(jnp.float32) + routed + shared_out).astype(jnp.bfloat16)
    return (layer_out, new_state)


def solution(mesh):
    in_specs = (
        P(("grp", "ep"), None),
        P(None, ("grp", "ep"), "tp"),
        P(),
        P(None, "tp"),
        P("tp", None),
        P("tp", None),
        P("tp"),
        P(None, "tp", None, None),
        P(None, "tp", None, None),
        P("tp"),
        P("tp", None),
        P(),
        P("ep", None, "tp"),
        P("ep", None, "tp"),
        P("ep", "tp", None),
        P(None, "tp"),
        P(None, "tp"),
        P("tp", None),
        P(("grp", "ep"), None),
        P(("grp", "ep"), None),
    )
    out_specs = (P(("grp", "ep"), "tp"), P(None, ("grp", "ep"), "tp"))
    return jax.shard_map(body, mesh=mesh, in_specs=in_specs, out_specs=out_specs, check_vma=False)
```
